256 devices in a mesh: grp: 2 (over y), ep: 32 (over z, core), tp: 4 (over x).
Axes of the slice: x: 4, y: 2, z: 16, core: 2. Of those that a mesh axis runs over, the one named last changes fastest.
The devices are a block of a 4x16x16 slice.
Arguments:
- mix_rows: bfloat16 [32768, 2048], P(('grp', 'ep', 'tp')), parts along dimension 0, may hold values from -6 to 6
- expert_rows: bfloat16 [32768, 2048], P(('grp', 'ep', 'tp')), parts along dimension 0, may hold values from -6 to 6
- mix_gain: float32 [2048], replicated, may hold values from 0.1 to 1.9
- ffn_gain: float32 [2048], replicated, may hold values from 0.1 to 1.9
- w_query: bfloat16 [2048, 512], P(None, 'tp'), may hold values from -0.125 to 0.125
- w_key: bfloat16 [2048, 512], P(None, 'tp'), may hold values from -0.125 to 0.125
- w_value: bfloat16 [2048, 1024], P(None, 'tp'), may hold values from -0.125 to 0.125
- w_lowrank: bfloat16 [2048, 32], replicated, may hold values from -0.125 to 0.125
- w_decay: bfloat16 [32, 512], replicated, may hold values from -1 to 1
- decay_bias: float32 [512], replicated, may hold values from -1.5 to 16
- decay_shift: float32 [8, 32768], P('tp', ('grp', 'ep')), parts along dimension 1, may hold values from -2 to 0
- head_gain: float32 [128], replicated, may hold values from 0.1 to 1.9
- w_output: bfloat16 [1024, 2048], P('tp'), may hold values from -0.1875 to 0.1875
- route_ids: int32 [32768, 4], P(('grp', 'ep', 'tp')), parts along dimension 0, may hold values from 0 to 127, all different within a row; in each aligned block of 128 rows (0 to 127, 128 to 255, ...) at most 8 rows name the same one
- route_weights: float32 [32768, 4], P(('grp', 'ep', 'tp')), parts along dimension 0, may hold values from 0.3 to 1.2
- w_gate: bfloat16 [128, 2048, 512], P(('ep', 'tp')), may hold values from -0.125 to 0.125
- w_lift: bfloat16 [128, 2048, 512], P(('ep', 'tp')), may hold values from -0.125 to 0.125
- w_drop: bfloat16 [128, 512, 2048], P(('ep', 'tp')), may hold values from -0.25 to 0.25
- shared_gate: bfloat16 [2048, 512], P(None, 'tp'), may hold values from -0.125 to 0.125
- shared_lift: bfloat16 [2048, 512], P(None, 'tp'), may hold values from -0.125 to 0.125
- shared_drop: bfloat16 [512, 2048], P('tp'), may hold values from -0.25 to 0.25
Outputs:
- mixed: bfloat16 [32768, 2048], P(('grp', 'ep', 'tp')), parts along dimension 0
- expert_out: bfloat16 [32768, 2048], P(('grp', 'ep', 'tp')), parts along dimension 0
The draws below stay inside these ranges and needn't reach their ends.
There are 2 independent parts, one for each index of `grp`. The reference program is written for one: setup_inputs(seed, part) draws one part's arguments, and reference() takes and returns one part's arrays. A program takes and returns all parts, laid end to end along the dimension named above; an argument that names none is the same for every part. Nothing has to cross between parts.
Inputs may be any that keep to these rules, and one draw needn't show every extreme that they name: `route_ids`: each row names 4 different experts. In each aligned block of 128 rows (the rows of one device) no expert is named by more than 8 rows.
All inputs are finite; a program needn't handle non-finite values.
Results may differ from the reference program's by a relative error of at most 0.014.
Values may be sent and summed in bfloat16 or wider, within the bound.
A program may use at most 128 MiB of HBM per device.

```python
import math
import jax
import jax.numpy as jnp
import numpy as np
from jax import lax

D = 2048
HEAD_COUNT = 8
DK = 64
DV = 128
LOWRANK = 32
BLOCK = 64
FF = 512
TOP_K = 4
TOK_DEV = 128
SPAN = 512
SEQUENCE_LENGTH = 16384
EXPERTS = 128
CAP = 8
N_EP = 32
N_TP = 4


def draw_decay_bias(key, part):
    key_sequence = jax.random.split(jax.random.fold_in(key, 7), 3)
    slow_share = 4
    slow_heads = jax.random.randint(key_sequence[0], (HEAD_COUNT,), 0, 8) < slow_share
    fast_bias = jax.random.uniform(key_sequence[1], (HEAD_COUNT, DK), jnp.float32, -1.5, 1.0)
    slow_floor = math.log(SEQUENCE_LENGTH) + 1.0
    slow_bias = slow_floor + jax.random.uniform(key_sequence[2], (HEAD_COUNT, DK), jnp.float32, 0.0, 1.0) * (16.0 - slow_floor)
    return jnp.where(slow_heads[:, None], slow_bias, fast_bias).reshape(HEAD_COUNT * DK).astype(jnp.float32)


def draw_decay_shift(key, part):
    key_sequence = jax.random.split(jax.random.fold_in(key, 13), 3)
    spans = SEQUENCE_LENGTH // SPAN
    factor = jnp.exp(jax.random.uniform(key_sequence[0], (HEAD_COUNT, spans), jnp.float32, math.log(0.4), math.log(2.5)))
    stable_level = jnp.repeat(factor, SPAN, axis=1) * (0.6 / SEQUENCE_LENGTH)
    spike_locations = jax.random.randint(key_sequence[1], (HEAD_COUNT, 3), 0, SEQUENCE_LENGTH)
    spike_depth = jax.random.uniform(key_sequence[2], (HEAD_COUNT, 3), jnp.float32, 0.22, 0.6)
    position_index = jnp.arange(SEQUENCE_LENGTH, dtype=jnp.int32)
    spike_hits = (position_index[None, None, :] == spike_locations[:, :, None]).astype(jnp.float32)
    spike_events = jnp.sum(spike_hits * spike_depth[:, :, None], axis=1)
    return (-(stable_level + spike_events)).astype(jnp.float32)


def steps_of(key, dims, pieces, least, high):
    loudness = 1.0
    for dim, blocks in pieces:
        heights = jax.random.uniform(jax.random.fold_in(jax.random.fold_in(key, 6), dim), (blocks,), jnp.float32, least / len(pieces), high / len(pieces))
        loudness = loudness * jnp.repeat(jnp.exp(heights), dims[dim] // blocks).reshape((-1,) + (1,) * (len(dims) - 1 - dim))
    return loudness


def shared_out(rng, own, number, rows, number_of, top, limit, skew):
    order = jax.random.permutation(rng, number_of)
    heavy_load, common = shares(number_of, rows * top, limit, skew, True), shares(number_of, rows * top, limit, skew, False)
    places = jnp.arange(number_of)

    def named(tallies, rotation):
        used = int((tallies > 0).sum())
        fixed = max(1, used // 4)
        moved = fixed + (places - fixed + rotation * (used - fixed)) % max(1, number_of - fixed)
        return jnp.zeros((number_of,), jnp.int32).at[order[jnp.where(places < fixed, places, moved)]].set(jnp.asarray(tallies, jnp.int32))

    tallies = jnp.where(number % 4 == 0, named(heavy_load, number // 4), named(common, number - number // 4 - 1))
    mixed = jax.random.permutation(jax.random.fold_in(own, 3), number_of)
    donor, taker = mixed[0:number_of // 2 * 2:2], mixed[1:number_of // 2 * 2:2]
    slack = jnp.minimum(tallies[donor] - 1, limit - tallies[taker]) // 2
    slack = jnp.where((donor == order[0]) | (taker == order[0]) | (tallies[taker] == 0), 0, jnp.maximum(slack, 0))
    moved = jax.random.randint(jax.random.fold_in(own, 4), (number_of // 2,), 0, 1 << 20) % (slack + 1)
    tallies = tallies.at[donor].add(-moved).at[taker].add(moved)
    labels = jnp.searchsorted(jnp.cumsum(tallies), jnp.arange(rows * top), side="right").astype(jnp.int32)
    grid = labels.reshape(top, rows).T
    grid = grid[jax.random.permutation(jax.random.fold_in(own, 1), rows)]
    rotation = jax.random.randint(jax.random.fold_in(own, 2), (rows, 1), 0, top)
    return jnp.take_along_axis(grid, (jnp.arange(top)[None, :] + rotation) % top, axis=1)


def shares(number_of, total, most, slope, full):
    weights = [(1 << 20) // math.isqrt(standing ** slope) + 1 for standing in range(1, number_of + 1)]
    largest = most if full else min(most, max(-(-total // number_of), total * weights[0] // sum(weights)))
    least = 1 if total - largest >= number_of - 1 else 0
    given, rest = [largest] + [least] * (number_of - 1), total - largest - least * (number_of - 1)
    while rest > 0:
        candidates = [i for i in range(1, number_of) if given[i] < largest] or [i for i in range(1, number_of) if given[i] < most]
        whole, remaining = sum([weights[i] for i in candidates]), rest
        for i in candidates:
            more = min(most - given[i], max(1, remaining * weights[i] // whole), rest)
            given[i] = given[i] + more
            rest = rest - more
    return np.array(given)


def normal_values(key, extent, scale, most, shards=(), held_as=jnp.bfloat16):
    factor_of = steps_of(key, extent, shards, -0.22, 0.18) if shards else 1.0
    drawn = jax.random.normal(key, extent, jnp.float32) * scale * factor_of
    return jnp.minimum(jnp.maximum(drawn, -most), most).astype(held_as)


def setup_inputs(seed: int = 0, part: int = 0) -> dict:
    streams_of = jax.random.split(jax.random.key(seed), 22)
    own_keys = jax.random.split(jax.random.fold_in(streams_of[21], part), 22)
    mix_rows = normal_values(own_keys[0], (SEQUENCE_LENGTH, D), 1.0, 6.0, ((0, 128),))
    expert_rows = normal_values(own_keys[1], (SEQUENCE_LENGTH, D), 1.0, 6.0, ((0, 128),))
    mix_gain = jnp.clip(1.0 + 0.18 * jax.random.normal(streams_of[2], (D,), jnp.float32), 0.1, 1.9)
    ffn_gain = jnp.clip(1.0 + 0.18 * jax.random.normal(streams_of[3], (D,), jnp.float32), 0.1, 1.9)
    w_query = normal_values(streams_of[4], (D, HEAD_COUNT * DK), D ** -0.5, 0.125, ((1, 4),))
    w_key = normal_values(streams_of[5], (D, HEAD_COUNT * DK), D ** -0.5, 0.125, ((1, 4),))
    w_value = normal_values(streams_of[6], (D, HEAD_COUNT * DV), D ** -0.5, 0.125, ((1, 4),))
    w_lowrank = normal_values(streams_of[7], (D, LOWRANK), D ** -0.5, 0.125)
    w_decay = normal_values(streams_of[8], (LOWRANK, HEAD_COUNT * DK), LOWRANK ** -0.5, 1.0)
    decay_bias = draw_decay_bias(jax.random.fold_in(streams_of[21], 71), part)
    decay_shift = draw_decay_shift(jax.random.fold_in(jax.random.fold_in(streams_of[21], part), 71), part)
    head_gain = jnp.clip(1.0 + 0.18 * jax.random.normal(streams_of[11], (DV,), jnp.float32), 0.1, 1.9)
    w_output = normal_values(streams_of[12], (HEAD_COUNT * DV, D), (HEAD_COUNT * DV) ** -0.5, 0.1875, ((0, 4),))
    route_ids_keys = jax.random.split(jax.random.fold_in(own_keys[13], 1), SEQUENCE_LENGTH // TOK_DEV)
    route_ids_turns = jax.random.permutation(jax.random.fold_in(own_keys[13], 3), SEQUENCE_LENGTH // TOK_DEV)
    route_ids = jax.vmap(lambda own, number: shared_out(jax.random.fold_in(own_keys[13], 2), own, number, TOK_DEV, EXPERTS, TOP_K, CAP, 2))(route_ids_keys, route_ids_turns).reshape((SEQUENCE_LENGTH, TOP_K))
    route_weights = jnp.clip(0.3 + 0.90000004 * jax.random.uniform(own_keys[14], (SEQUENCE_LENGTH, TOP_K), jnp.float32) ** steps_of(own_keys[14], (SEQUENCE_LENGTH, TOP_K), ((0, 128),), -0.2, 0.2), 0.3, 1.2)
    w_gate = normal_values(streams_of[15], (EXPERTS, D, FF), D ** -0.5, 0.125, ((0, 128),))
    w_lift = normal_values(streams_of[16], (EXPERTS, D, FF), D ** -0.5, 0.125, ((0, 128),))
    w_drop = normal_values(streams_of[17], (EXPERTS, FF, D), FF ** -0.5, 0.25, ((0, 128),))
    shared_gate = normal_values(streams_of[18], (D, FF), D ** -0.5, 0.125, ((1, 4),))
    shared_lift = normal_values(streams_of[19], (D, FF), D ** -0.5, 0.125, ((1, 4),))
    shared_drop = normal_values(streams_of[20], (FF, D), FF ** -0.5, 0.25, ((0, 4),))
    return {"mix_rows": mix_rows, "expert_rows": expert_rows, "mix_gain": mix_gain, "ffn_gain": ffn_gain, "w_query": w_query, "w_key": w_key, "w_value": w_value, "w_lowrank": w_lowrank, "w_decay": w_decay, "decay_bias": decay_bias, "decay_shift": decay_shift, "head_gain": head_gain, "w_output": w_output, "route_ids": route_ids, "route_weights": route_weights, "w_gate": w_gate, "w_lift": w_lift, "w_drop": w_drop, "shared_gate": shared_gate, "shared_lift": shared_lift, "shared_drop": shared_drop}


epsilon = 1e-05
gate_norm = 16.0
highest = lax.Precision.HIGHEST

def layer_norm(source, gain):
    values = source.astype(jnp.float32)
    center = values - lax.optimization_barrier(jnp.mean(values, axis=-1, keepdims=True))
    inverse = lax.rsqrt(lax.optimization_barrier(jnp.mean(center * center, axis=-1, keepdims=True)) + epsilon)
    return (center * inverse * gain).astype(jnp.bfloat16)

def stored(product):
    return lax.optimization_barrier(product.astype(jnp.bfloat16)).astype(jnp.float32)

def head_norm(attended, head_gain):
    inverse = lax.rsqrt(lax.optimization_barrier(jnp.mean(attended * attended, axis=-1, keepdims=True)) + epsilon)
    return (attended * inverse * head_gain).astype(jnp.bfloat16)

def gla_blocks(queries, key_rows, value_rows, log_decay, state_init):
    length, heads_here, key_width = queries.shape
    value_width = value_rows.shape[-1]
    blocks = length // BLOCK
    query_blocks = queries.reshape(blocks, BLOCK, heads_here, key_width)
    key_blocks = key_rows.reshape(blocks, BLOCK, heads_here, key_width)
    value_blocks = value_rows.reshape(blocks, BLOCK, heads_here, value_width)
    within = jnp.cumsum(log_decay.reshape(blocks, BLOCK, heads_here, key_width), axis=1)
    block_total = within[:, -1]
    scaled_query = query_blocks * jnp.exp(within)
    scaled_key = key_blocks * jnp.exp(-within)
    causal = jnp.tril(jnp.ones((BLOCK, BLOCK), dtype=jnp.bool_))
    scores = jnp.einsum('nihd,njhd->nhij', scaled_query, scaled_key, precision=highest)
    scores = jnp.where(causal, scores, 0.0)
    inside = jnp.einsum('nhij,njhv->nihv', scores, value_blocks, precision=highest)
    block_added = jnp.einsum('njhd,njhv->nhdv', key_blocks * jnp.exp(block_total[:, None] - within), value_blocks, precision=highest)

    def advance(state, inputs):
        decay_sum, addition = inputs
        return (jnp.exp(decay_sum)[:, :, None] * state + addition, state)
    final_state, entering = lax.scan(advance, state_init, (block_total, block_added))
    inside = inside + jnp.einsum('nihd,nhdv->nihv', scaled_query, entering, precision=highest)
    before = jnp.cumsum(block_total, axis=0) - block_total
    carried_query = query_blocks * jnp.exp(within + before[:, None])
    return (inside.reshape(length, heads_here, value_width), final_state, carried_query.reshape(length, heads_here, key_width), lax.optimization_barrier(jnp.sum(block_total, axis=0)))

def reference(mix_rows, expert_rows, mix_gain, ffn_gain, w_query, w_key, w_value, w_lowrank, w_decay, decay_bias, decay_shift, head_gain, w_output, route_ids, route_weights, w_gate, w_lift, w_drop, shared_gate, shared_lift, shared_drop):
    mix_normed = layer_norm(mix_rows, mix_gain)
    length = mix_normed.shape[0]
    queries = stored(jnp.dot(mix_normed, w_query, preferred_element_type=jnp.float32)).reshape(length, HEAD_COUNT, DK) * DK ** (-0.5)
    key_rows = stored(jnp.dot(mix_normed, w_key, preferred_element_type=jnp.float32)).reshape(length, HEAD_COUNT, DK)
    value_rows = stored(jnp.dot(mix_normed, w_value, preferred_element_type=jnp.float32)).reshape(length, HEAD_COUNT, DV)
    lowrank = jnp.dot(mix_normed, w_lowrank, preferred_element_type=jnp.float32).astype(jnp.bfloat16)
    logits = jnp.dot(lowrank, w_decay, preferred_element_type=jnp.float32) + decay_bias
    log_decay = jax.nn.log_sigmoid(logits).reshape(length, HEAD_COUNT, DK) / gate_norm + jnp.transpose(decay_shift)[:, :, None]
    gla_result = gla_blocks(queries, key_rows, value_rows, log_decay, jnp.zeros((HEAD_COUNT, DK, DV), jnp.float32))
    head_rows = head_norm(gla_result[0], head_gain).reshape(length, HEAD_COUNT * DV)
    group_width = HEAD_COUNT // N_TP * DV
    mixed = jnp.zeros((length, D), jnp.float32)
    for group_index in range(N_TP):
        first_row = group_index * group_width
        group_term = jnp.dot(head_rows[:, first_row:first_row + group_width], w_output[first_row:first_row + group_width], preferred_element_type=jnp.float32)
        mixed = mixed + group_term.astype(jnp.bfloat16).astype(jnp.float32)
    mixed = mixed.astype(jnp.bfloat16)
    expert_normed = layer_norm(expert_rows, ffn_gain)
    shared_hidden = (jax.nn.silu(jnp.dot(expert_normed, shared_gate, preferred_element_type=jnp.float32)) * jnp.dot(expert_normed, shared_lift, preferred_element_type=jnp.float32)).astype(jnp.bfloat16)
    unit_width = FF // N_TP
    shared_sum = jnp.zeros((length, D), jnp.float32)
    for group_index in range(N_TP):
        first_unit = group_index * unit_width
        unit_term = jnp.dot(shared_hidden[:, first_unit:first_unit + unit_width], shared_drop[first_unit:first_unit + unit_width], preferred_element_type=jnp.float32)
        shared_sum = shared_sum + unit_term.astype(jnp.bfloat16).astype(jnp.float32)
    flat_routes = route_ids.reshape(-1).astype(jnp.int32)
    expert_ids = jnp.arange(EXPERTS, dtype=jnp.int32)
    matches = (flat_routes[:, None] == expert_ids[None, :]).astype(jnp.int32)
    slot_rank = lax.optimization_barrier(jnp.sum((jnp.cumsum(matches, axis=0) - 1) * matches, axis=1)).astype(jnp.int32)
    slot_count = CAP * N_EP * N_TP
    token_index = jnp.arange(length * TOP_K, dtype=jnp.int32) // TOP_K
    slot_token = jnp.full((EXPERTS, slot_count), length, jnp.int32).at[flat_routes, slot_rank].set(token_index)
    slot_weight = jnp.zeros((EXPERTS, slot_count), jnp.float32).at[flat_routes, slot_rank].set(route_weights.reshape(-1).astype(jnp.float32))
    padded = jnp.concatenate([expert_normed, jnp.zeros((1, D), jnp.bfloat16)], axis=0)

    def one_expert(summed, inputs):
        token_slots, weight_slots, gate_matrix, lift_matrix, drop_matrix = inputs
        gathered = padded[token_slots]
        inner = (jax.nn.silu(jnp.dot(gathered, gate_matrix, preferred_element_type=jnp.float32)) * jnp.dot(gathered, lift_matrix, preferred_element_type=jnp.float32)).astype(jnp.bfloat16)
        result = stored(jnp.dot(inner, drop_matrix, preferred_element_type=jnp.float32))
        return (summed.at[token_slots].add(weight_slots[:, None] * result), None)
    routed, unused = lax.scan(one_expert, jnp.zeros((length + 1, D), jnp.float32), (slot_token, slot_weight, w_gate, w_lift, w_drop))
    expert_out = (shared_sum + routed[:length]).astype(jnp.bfloat16)
    return (mixed, expert_out)
```

```python
import functools

import jax
import jax.numpy as jnp
from jax import lax
from jax.experimental import pallas as pl
from jax.experimental.pallas import tpu as pltpu
from jax.sharding import Mesh
from jax.sharding import PartitionSpec as P

DK = 64
DV = 128
BLOCK = 64
EP = ("ep_0", "ep_1")
EP_TP = ("ep_0", "ep_1", "tp")
GRP_EP_TP = ("grp", "ep_0", "ep_1", "tp")
GRP_EP = ("grp", "ep_0", "ep_1")


epsilon = 1e-05
gate_norm = 16.0
highest = lax.Precision.HIGHEST


def filled_with(value, identity):
    return jax.tree.map(
        lambda a, e: jnp.broadcast_to(jnp.asarray(e, a.dtype), a.shape), value, identity
    )


def gathered_once(value, axis):
    leaves = jax.tree.leaves(value)
    sequence = sorted(range(len(leaves)), key=lambda k: -leaves[k].size)
    width = (1, *leaves[sequence[0]].shape)[-1]
    lines = [
        jnp.pad(leaves[k].reshape(-1), (0, -leaves[k].size % width)).reshape(-1, width)
        for k in sequence
    ]
    both, at, found = (lax.all_gather(jnp.concatenate(lines), axis), 0, {})
    for k, line in zip(sequence, lines):
        share = both[:, at : at + len(line)].reshape(len(both), -1)
        found[k] = share[:, : leaves[k].size].reshape(-1, *leaves[k].shape)
        at += len(line)
    numbers = iter(range(len(leaves)))
    return jax.tree.map(lambda _: found[next(numbers)], value)


def carried_in(value, axes, combine, identity):
    before = start = filled_with(value, identity)
    total = value
    for axis in reversed(axes):
        length, mine = (lax.axis_size(axis), lax.axis_index(axis))
        pieces = gathered_once(
            jax.tree.map(lambda part, kind: part.astype(kind), total, (jnp.bfloat16, jnp.bfloat16)),
            axis,
        )
        inside, total = (start, start)
        for k in range(length):
            passed = k < mine
            total = combine(
                total, jax.tree.map(lambda part, own: part[k].astype(own.dtype), pieces, value)
            )
            inside = jax.tree.map(lambda new, old: jnp.where(passed, new, old), total, inside)
        before = combine(inside, before)
    return before


def layer_norm(source, gain):
    values = source.astype(jnp.float32)
    center = values - jnp.mean(values, axis=-1, keepdims=True)
    inverse = lax.rsqrt(jnp.mean(center * center, axis=-1, keepdims=True) + epsilon)
    return (center * inverse * gain).astype(jnp.bfloat16)


def stored(product):
    return lax.optimization_barrier(product.astype(jnp.bfloat16)).astype(jnp.float32)


def gla_blocks(queries, key_rows, value_rows, log_decay, state_init):
    length, heads_here, key_width = queries.shape
    value_width = value_rows.shape[-1]
    blocks = length // BLOCK
    query_blocks = queries.reshape(blocks, BLOCK, heads_here, key_width)
    key_blocks = key_rows.reshape(blocks, BLOCK, heads_here, key_width)
    value_blocks = value_rows.reshape(blocks, BLOCK, heads_here, value_width)
    within = jnp.cumsum(log_decay.reshape(blocks, BLOCK, heads_here, key_width), axis=1)
    block_total = within[:, -1]
    scaled_query = query_blocks * jnp.exp(within)
    scaled_key = key_blocks * jnp.exp(-within)
    causal = jnp.tril(jnp.ones((BLOCK, BLOCK), dtype=jnp.bool_))
    scores = jnp.einsum("nihd,njhd->nhij", scaled_query, scaled_key, precision=highest)
    scores = jnp.where(causal, scores, 0.0)
    inside = jnp.einsum("nhij,njhv->nihv", scores, value_blocks, precision=highest)
    block_added = jnp.einsum(
        "njhd,njhv->nhdv",
        key_blocks * jnp.exp(block_total[:, None] - within),
        value_blocks,
        precision=highest,
    )

    def advance(state, inputs):
        decay_sum, addition = inputs
        return (jnp.exp(decay_sum)[:, :, None] * state + addition, state)

    final_state, entering = lax.scan(advance, state_init, (block_total, block_added))
    inside = inside + jnp.einsum("nihd,nhdv->nihv", scaled_query, entering, precision=highest)
    before = jnp.cumsum(block_total, axis=0) - block_total
    carried_query = query_blocks * jnp.exp(within + before[:, None])
    return (
        inside.reshape(length, heads_here, value_width),
        final_state,
        carried_query.reshape(length, heads_here, key_width),
        jnp.sum(block_total, axis=0),
    )


MESH = pl.DeviceIdType.MESH


def plane_rows(values, width):
    return jnp.concatenate(
        [jnp.broadcast_to(values[j : j + 1], (width, values.shape[1])) for j in range(len(values))],
        axis=0,
    )


def moe_kernel(
    nz, nc, nx,
    rows_ref, meta_ref, gate_hbm, lift_hbm, drop_hbm,
    out_ref,
    held, metas, picks, outgoing, arrived, results, back, sums, first,
    gate_ref, lift_ref, drop_ref, hidden, own_sum,
    ag_send, ag_recv, meta_send, meta_recv, out_send, out_recv, back_send, back_recv,
    rs_send, rs_recv, load_sem,
):
    half = nz // 2
    peers = nc * nx
    z = lax.axis_index("ep_0")
    core = lax.axis_index("ep_1")
    col = lax.axis_index("tp")
    me = core * nx + col
    tokens, width = rows_ref.shape
    cut = width // 2
    slots = arrived.shape[1] // peers
    cap = slots // 2
    right, left = lax.rem(z + 1, nz), lax.rem(z + nz - 1, nz)
    beside = (right, left)

    def peer(i):
        number = lax.rem(me + i, peers)
        return number, {"ep_1": number // nx, "tp": lax.rem(number, nx)}

    barrier = pltpu.get_barrier_semaphore()
    for neighbour in beside:
        pl.semaphore_signal(barrier, inc=1, device_id={"ep_0": neighbour}, device_id_type=MESH)
    for i in range(1, peers):
        pl.semaphore_signal(barrier, inc=1, device_id=peer(i)[1], device_id_type=MESH)
    loads = [
        pltpu.make_async_copy(a, b, load_sem.at[k])
        for k, (a, b) in enumerate(
            ((gate_hbm, gate_ref), (lift_hbm, lift_ref), (drop_hbm, drop_ref))
        )
    ]
    for load in loads:
        load.start()
    held[0, 0:tokens] = rows_ref[...]
    metas[0, 0:8] = meta_ref[...]
    pl.semaphore_wait(barrier, peers + 1)

    def place(k, way):
        if isinstance(k, int) and k == half:
            return 0, slice(tokens, 2 * tokens)
        return k, slice(0, tokens) if way == 0 else slice(tokens, 2 * tokens)

    def columns(c):
        return slice(c * cut, (c + 1) * cut)

    def gather_copy(k, way, c):
        if isinstance(k, int) and k == 1:
            source = rows_ref.at[:, columns(c)]
        else:
            at, span = place(k - 1, way)
            source = held.at[at, span, columns(c)]
        at, span = place(k, way)
        return pltpu.make_async_remote_copy(
            source, held.at[at, span, columns(c)],
            ag_send.at[way, k, c], ag_recv.at[way, k, c],
            device_id={"ep_0": beside[way]}, device_id_type=MESH,
        )

    def meta_place(k, way):
        if isinstance(k, int) and k == half:
            return 0, slice(8, 16)
        return k, slice(0, 8) if way == 0 else slice(8, 16)

    def meta_copy(k, way):
        if isinstance(k, int) and k == 1:
            source = meta_ref
        else:
            at, span = meta_place(k - 1, way)
            source = metas.at[at, span]
        at, span = meta_place(k, way)
        return pltpu.make_async_remote_copy(
            source, metas.at[at, span], meta_send.at[way, k], meta_recv.at[way, k],
            device_id={"ep_0": beside[way]}, device_id_type=MESH,
        )

    def block(number):
        return pl.ds(pl.multiple_of(number * slots, slots), slots)

    def out_copy(k, i):
        number, there = peer(i)
        return pltpu.make_async_remote_copy(
            outgoing.at[k, block(number)], arrived.at[k, block(me)],
            out_send.at[k, i], out_recv.at[k, i], device_id=there, device_id_type=MESH,
        )

    def out_landed(k, i):
        number, there = peer(peers - i)
        return pltpu.make_async_remote_copy(
            outgoing.at[k, block(number)], arrived.at[k, block(number)],
            out_send.at[k, i], out_recv.at[k, i], device_id=there, device_id_type=MESH,
        )

    def back_copy(k, i):
        number, there = peer(i)
        return pltpu.make_async_remote_copy(
            results.at[k, block(number)], back.at[k, block(me)],
            back_send.at[k, i], back_recv.at[k, i], device_id=there, device_id_type=MESH,
        )

    def back_landed(k, i):
        number, there = peer(peers - i)
        return pltpu.make_async_remote_copy(
            results.at[k, block(number)], back.at[k, block(number)],
            back_send.at[k, i], back_recv.at[k, i], device_id=there, device_id_type=MESH,
        )

    experts = (z * peers + lax.broadcasted_iota(jnp.int32, (peers, tokens), 0)).astype(jnp.float32)
    earlier = (
        lax.broadcasted_iota(jnp.int32, (tokens, tokens), 0)
        < lax.broadcasted_iota(jnp.int32, (tokens, tokens), 1)
    ).astype(jnp.bfloat16)
    line = lax.broadcasted_iota(jnp.int32, (peers * slots, tokens), 0)
    slot_of = lax.rem(line, cap).astype(jnp.float32)
    side_of = lax.rem(line // cap, 2)

    def dispatch(k):
        meta = metas[k]
        chosen, weighted = [], []
        for side in range(2):
            hits = jnp.zeros((peers, tokens), jnp.float32)
            weights = jnp.zeros((peers, tokens), jnp.float32)
            for choice in range(4):
                row = meta[side * 8 + choice : side * 8 + choice + 1]
                weight = meta[side * 8 + 4 + choice : side * 8 + 5 + choice]
                hit = jnp.where(row == experts, 1.0, 0.0)
                hits = hits + hit
                weights = weights + hit * weight
            rank = jnp.dot(
                hits.astype(jnp.bfloat16), earlier, preferred_element_type=jnp.float32
            )
            rank = jnp.where(hits > 0.5, rank, -1.0)
            match = (plane_rows(rank, slots) == slot_of) & (side_of == side)
            chosen.append(jnp.where(match, 1.0, 0.0))
            weighted.append(jnp.where(match, plane_rows(weights, slots), 0.0))
        picks[k] = jnp.concatenate(weighted, axis=1).astype(jnp.bfloat16)
        choose = jnp.concatenate(chosen, axis=1).astype(jnp.bfloat16)
        tile = 512

        @pl.loop(0, width // tile)
        def _(n):
            span = pl.ds(pl.multiple_of(n * tile, tile), tile)
            outgoing[k, :, span] = jnp.dot(
                choose, held[k, :, span], preferred_element_type=jnp.float32
            ).astype(jnp.bfloat16)

        for i in range(1, peers):
            out_copy(k, i).start()
        arrived[k, block(me)] = outgoing[k, block(me)]

    def experts_on(k):
        for i in range(1, peers):
            out_landed(k, i).wait_recv()
        tile = 256

        @pl.loop(0, hidden.shape[1] // tile)
        def _(n):
            span = pl.ds(pl.multiple_of(n * tile, tile), tile)
            gate = jnp.dot(arrived[k], gate_ref[:, span], preferred_element_type=jnp.float32)
            lift = jnp.dot(arrived[k], lift_ref[:, span], preferred_element_type=jnp.float32)
            hidden[:, span] = (gate / (1.0 + jnp.exp(-gate)) * lift).astype(jnp.bfloat16)

        @pl.loop(0, width // tile)
        def _(n):
            span = pl.ds(pl.multiple_of(n * tile, tile), tile)
            results[k, :, span] = jnp.dot(
                hidden[...], drop_ref[:, span], preferred_element_type=jnp.float32
            ).astype(jnp.bfloat16)

        for i in range(1, peers):
            back_copy(k, i).start()
        back[k, block(me)] = results[k, block(me)]

    for c in range(2):
        for way in range(2):
            gather_copy(1, way, c).start()
    for way in range(2):
        meta_copy(1, way).start()

    def step(k):
        for c in range(2):
            for way in range(2):
                gather_copy(k, way, c).wait_recv()
                gather_copy(k + 1, way, c).start()
        for way in range(2):
            meta_copy(k, way).wait_recv()
            meta_copy(k + 1, way).start()
        dispatch(k)

    for c in range(2):
        for way in range(2):
            gather_copy(1, way, c).wait_recv()
            gather_copy(2, way, c).start()
    for way in range(2):
        meta_copy(1, way).wait_recv()
        meta_copy(2, way).start()
    dispatch(1)
    for load in loads:
        load.wait()

    @pl.loop(2, half - 1)
    def _(k):
        step(k)
        experts_on(k - 1)

    last = half - 1
    for c in range(2):
        for way in range(2):
            gather_copy(last, way, c).wait_recv()
            if way == c:
                gather_copy(half, way, c).start()
    for way in range(2):
        meta_copy(last, way).wait_recv()
    meta_copy(half, 0).start()
    dispatch(last)
    experts_on(last - 1)
    for c in range(2):
        gather_copy(half, c, c).wait_recv()
    meta_copy(half, 0).wait_recv()
    dispatch(0)
    experts_on(last)
    experts_on(0)

    def combined(k, span):
        return lax.dot_general(
            picks[k], back[k, :, span], (((0,), (0,)), ((), ())),
            preferred_element_type=jnp.float32,
        )

    def returned(k):
        for i in range(1, peers):
            back_landed(k, i).wait_recv()

    def sum_copy(k, way, c):
        if isinstance(k, int) and k == half:
            source = first.at[:, columns(c)]
        else:
            source = sums.at[way, k, :, columns(c)]
        return pltpu.make_async_remote_copy(
            source, sums.at[way, k - 1, :, columns(c)],
            rs_send.at[way, k, c], rs_recv.at[way, k, c],
            device_id={"ep_0": beside[way]}, device_id_type=MESH,
        )

    returned(0)
    for c in range(2):
        both = combined(0, columns(c))
        own_sum[:, columns(c)] = both[0:tokens]
        first[:, columns(c)] = both[tokens:].astype(jnp.bfloat16)
        sum_copy(half, c, c).start()

    def pass_on(k, c, landed):
        both = combined(k, columns(c))
        for way in range(2):
            part = both[tokens:] if way == 0 else both[0:tokens]
            if landed(way, c):
                sum_copy(k + 1, way, c).wait_recv()
                part = part + sums[way, k, :, columns(c)].astype(jnp.float32)
            sums[way, k, :, columns(c)] = part.astype(jnp.bfloat16)
            sum_copy(k, way, c).start()

    returned(last)
    for c in range(2):
        pass_on(last, c, lambda way, c: way == c)

    @pl.loop(1, last)
    def _(n):
        k = last - n
        returned(k)
        for c in range(2):
            pass_on(k, c, lambda way, c: True)

    for c in range(2):
        total = own_sum[:, columns(c)]
        for way in range(2):
            sum_copy(1, way, c).wait_recv()
            total = total + sums[way, 0, :, columns(c)].astype(jnp.float32)
        out_ref[:, columns(c)] = total

    for c in range(2):
        for way in range(2):
            gather_copy(1, way, c).wait_send()
            sum_copy(1, way, c).wait_send()
            if way == c:
                gather_copy(half, way, c).wait_send()
                sum_copy(half, way, c).wait_send()
    for way in range(2):
        meta_copy(1, way).wait_send()
    meta_copy(half, 0).wait_send()

    @pl.loop(2, half)
    def _(k):
        for way in range(2):
            for c in range(2):
                gather_copy(k, way, c).wait_send()
                sum_copy(k, way, c).wait_send()
            meta_copy(k, way).wait_send()

    @pl.loop(0, half)
    def _(k):
        for i in range(1, peers):
            out_copy(k, i).wait_send()
            back_copy(k, i).wait_send()


def routed(mesh_sizes, rows, ids, weights, w_gate, w_lift, w_drop):
    nz, nc, nx = mesh_sizes
    half, peers = nz // 2, nc * nx
    tokens, width = rows.shape
    ff = w_gate.shape[-1]
    cap = 2 * tokens * ids.shape[1] // (nz * peers)
    slots = 2 * cap
    meta = jnp.concatenate([ids.T.astype(jnp.float32), weights.T], axis=0)
    vmem, dma = pltpu.VMEM, pltpu.SemaphoreType.DMA
    bf = jnp.bfloat16
    whole = pl.BlockSpec(memory_space=pltpu.VMEM)
    anywhere = pl.BlockSpec(memory_space=pl.ANY)
    return pl.pallas_call(
        functools.partial(moe_kernel, nz, nc, nx),
        out_shape=jax.ShapeDtypeStruct((tokens, width), jnp.float32),
        in_specs=[whole, whole, anywhere, anywhere, anywhere],
        out_specs=whole,
        scratch_shapes=[
            vmem((half, 2 * tokens, width), bf),
            vmem((half, 16, tokens), jnp.float32),
            vmem((half, peers * slots, 2 * tokens), bf),
            vmem((half, peers * slots, width), bf),
            vmem((half, peers * slots, width), bf),
            vmem((half, peers * slots, width), bf),
            vmem((half, peers * slots, width), bf),
            vmem((2, half, tokens, width), bf),
            vmem((tokens, width), bf),
            vmem((width, ff), bf),
            vmem((width, ff), bf),
            vmem((ff, width), bf),
            vmem((peers * slots, ff), bf),
            vmem((tokens, width), jnp.float32),
            dma((2, half + 1, 2)), dma((2, half + 1, 2)),
            dma((2, half + 1)), dma((2, half + 1)),
            dma((half, peers)), dma((half, peers)),
            dma((half, peers)), dma((half, peers)),
            dma((2, half + 1, 2)), dma((2, half + 1, 2)),
            dma((3,)),
        ],
        compiler_params=pltpu.CompilerParams(
            collective_id=0, has_side_effects=True, vmem_limit_bytes=58 * 1024 * 1024
        ),
        cost_estimate=pl.CostEstimate(
            flops=200_000_000_000, bytes_accessed=16 * 2**20, transcendentals=0
        ),
    )(rows, meta, w_gate[0], w_lift[0], w_drop[0])


def body(
    mix_rows,
    expert_rows,
    mix_gain,
    ffn_gain,
    w_query,
    w_key,
    w_value,
    w_lowrank,
    w_decay,
    decay_bias,
    decay_shift,
    head_gain,
    w_output,
    route_ids,
    route_weights,
    w_gate,
    w_lift,
    w_drop,
    shared_gate,
    shared_lift,
    shared_drop,
):
    mix_normed = layer_norm(mix_rows, mix_gain)
    local_heads = w_query.shape[1] // DK
    key_cols = local_heads * DK
    value_cols = w_value.shape[1]
    column = lax.axis_index("tp") * key_cols
    decay_cols = lax.dynamic_slice_in_dim(w_decay, column, key_cols, 1)
    bias_cols = lax.dynamic_slice_in_dim(decay_bias, column, key_cols, 0)
    shard_rows = lax.all_gather(mix_normed, "tp", axis=0, tiled=True)
    query_part = jnp.dot(shard_rows, w_query, preferred_element_type=jnp.float32)
    key_part = jnp.dot(shard_rows, w_key, preferred_element_type=jnp.float32)
    value_part = jnp.dot(shard_rows, w_value, preferred_element_type=jnp.float32)
    lowrank = jnp.dot(shard_rows, w_lowrank, preferred_element_type=jnp.float32).astype(
        jnp.bfloat16
    )
    logits = jnp.dot(lowrank, decay_cols, preferred_element_type=jnp.float32) + bias_cols
    projected = jnp.concatenate(
        [stored(query_part), stored(key_part), stored(value_part), logits], axis=1
    )
    span_rows = projected.shape[0]
    queries = projected[:, :key_cols].reshape(span_rows, local_heads, DK) * DK ** (-0.5)
    key_rows = projected[:, key_cols : 2 * key_cols].reshape(span_rows, local_heads, DK)
    value_rows = projected[:, 2 * key_cols : 2 * key_cols + value_cols].reshape(
        span_rows, local_heads, DV
    )
    log_decay = (
        jax.nn.log_sigmoid(projected[:, 2 * key_cols + value_cols :]).reshape(
            span_rows, local_heads, DK
        )
        / gate_norm
        + jnp.transpose(decay_shift)[:, :, None]
    )
    zero_state = jnp.zeros((local_heads, DK, DV), jnp.float32)
    inside, final_state, carried_query, decay_total = gla_blocks(
        queries, key_rows, value_rows, log_decay, zero_state
    )

    def chain(earlier, later):
        return (earlier[0] + later[0], jnp.exp(later[0])[:, :, None] * earlier[1] + later[1])

    carried = carried_in(
        (decay_total, final_state), EP, chain, (jnp.zeros_like(decay_total), zero_state)
    )
    entering = carried[1]
    attended = inside + jnp.einsum("rhd,hdv->rhv", carried_query, entering, precision=highest)
    inverse = lax.rsqrt(jnp.mean(attended * attended, axis=-1, keepdims=True) + epsilon)
    head_rows = (
        (attended * inverse * head_gain).astype(jnp.bfloat16).reshape(span_rows, local_heads * DV)
    )
    mixed = lax.psum_scatter(
        jnp.dot(head_rows, w_output, preferred_element_type=jnp.float32).astype(jnp.bfloat16),
        "tp",
        scatter_dimension=0,
        tiled=True,
    )
    expert_normed = layer_norm(expert_rows, ffn_gain)
    shard_rows = lax.all_gather(expert_normed, "tp", axis=0, tiled=True)
    hidden = (
        jax.nn.silu(jnp.dot(shard_rows, shared_gate, preferred_element_type=jnp.float32))
        * jnp.dot(shard_rows, shared_lift, preferred_element_type=jnp.float32)
    ).astype(jnp.bfloat16)
    shared_sum = lax.psum_scatter(
        jnp.dot(hidden, shared_drop, preferred_element_type=jnp.float32).astype(jnp.bfloat16),
        "tp",
        scatter_dimension=0,
        tiled=True,
    ).astype(jnp.float32)
    sizes = (lax.axis_size("ep_0"), lax.axis_size("ep_1"), lax.axis_size("tp"))
    combined = shared_sum + routed(
        sizes, expert_normed, route_ids, route_weights, w_gate, w_lift, w_drop
    )
    return (mixed, combined.astype(jnp.bfloat16))


def solution(mesh):
    finer = Mesh(
        mesh.devices.reshape(mesh.shape["grp"], 16, 2, mesh.shape["tp"]),
        ("grp", "ep_0", "ep_1", "tp"),
    )
    in_specs = (
        P(GRP_EP_TP, None),
        P(GRP_EP_TP, None),
        P(),
        P(),
        P(None, "tp"),
        P(None, "tp"),
        P(None, "tp"),
        P(),
        P(),
        P(),
        P("tp", GRP_EP),
        P(),
        P("tp", None),
        P(GRP_EP_TP, None),
        P(GRP_EP_TP, None),
        P(EP_TP, None, None),
        P(EP_TP, None, None),
        P(EP_TP, None, None),
        P(None, "tp"),
        P(None, "tp"),
        P("tp", None),
    )
    out_specs = (P(GRP_EP_TP, None), P(GRP_EP_TP, None))
    return jax.shard_map(body, mesh=finer, in_specs=in_specs, out_specs=out_specs, check_vma=False)
```

```python
import functools

import jax
import jax.numpy as jnp
from jax import lax
from jax.experimental import pallas as pl
from jax.experimental.pallas import tpu as pltpu
from jax.sharding import Mesh
from jax.sharding import PartitionSpec as P

DK = 64
DV = 128
BLOCK = 64
EP = ("ep_0", "ep_1")
EP_TP = ("ep_0", "ep_1", "tp")
GRP_EP_TP = ("grp", "ep_0", "ep_1", "tp")
GRP_EP = ("grp", "ep_0", "ep_1")


epsilon = 1e-05
gate_norm = 16.0
highest = lax.Precision.HIGHEST


def layer_norm(source, gain):
    values = source.astype(jnp.float32)
    center = values - jnp.mean(values, axis=-1, keepdims=True)
    inverse = lax.rsqrt(jnp.mean(center * center, axis=-1, keepdims=True) + epsilon)
    return (center * inverse * gain).astype(jnp.bfloat16)


MESH = pl.DeviceIdType.MESH


def plane_rows(values, width):
    return jnp.concatenate(
        [jnp.broadcast_to(values[j : j + 1], (width, values.shape[1])) for j in range(len(values))],
        axis=0,
    )


def moe_kernel(
    nz, nc, nx,
    mix_ref, rows_ref, meta_ref, shift_ref, decay_ref, bias_ref, gain_ref,
    gate_hbm, lift_hbm, drop_hbm, query_hbm, key_hbm, value_hbm, low_hbm, mixout_hbm,
    sgate_hbm, slift_hbm, sdrop_hbm,
    mixed_ref, out_ref,
    held, metas, picks, outgoing, arrived, results, back, sums, first,
    gate_ref, lift_ref, drop_ref, query_ref, key_ref, value_ref, low_ref, mixout_ref,
    sgate_ref, slift_ref, sdrop_ref, hidden, own_sum,
    mix_all, exp_all, exp_part, mix_sums, exp_sums,
    q_rows, k_rows, v_rows, decays, inner, carried, state, before,
    chip_state, chip_total, mate_state, mate_total, prefix, prefix_total,
    scan_out, scan_total_out, scan_in, scan_total_in, entering,
    ag_send, ag_recv, meta_send, meta_recv, out_send, out_recv, back_send, back_recv,
    rs_send, rs_recv, load_sem,
    xg_send, xg_recv, xr_send, xr_recv, mate_send, mate_recv, scan_send, scan_recv,
):
    half = nz // 2
    peers = nc * nx
    mix_part = mix_all
    z = lax.axis_index("ep_0")
    core = lax.axis_index("ep_1")
    col = lax.axis_index("tp")
    me = core * nx + col
    tokens, width = rows_ref.shape
    cut = width // 2
    slots = arrived.shape[1] // peers
    cap = slots // 2
    right, left = lax.rem(z + 1, nz), lax.rem(z + nz - 1, nz)
    beside = (right, left)

    def peer(i):
        number = lax.rem(me + i, peers)
        return number, {"ep_1": number // nx, "tp": lax.rem(number, nx)}

    barrier = pltpu.get_barrier_semaphore()
    reaches = [d for d in (1, 2, 4, 8, 16, 32) if d < nz]
    near = sorted({d % nz for d in reaches} | {-d % nz for d in reaches})
    for d in near:
        there = {"ep_0": lax.rem(z + d, nz)}
        pl.semaphore_signal(barrier, inc=1, device_id=there, device_id_type=MESH)
    for i in range(1, peers):
        pl.semaphore_signal(barrier, inc=1, device_id=peer(i)[1], device_id_type=MESH)
    loads = [
        pltpu.make_async_copy(a, b, load_sem.at[k])
        for k, (a, b) in enumerate(
            (
                (query_hbm, query_ref), (key_hbm, key_ref), (value_hbm, value_ref),
                (low_hbm, low_ref), (gate_hbm, gate_ref), (lift_hbm, lift_ref),
                (drop_hbm, drop_ref), (sgate_hbm, sgate_ref), (slift_hbm, slift_ref),
                (sdrop_hbm, sdrop_ref), (mixout_hbm, mixout_ref),
            )
        )
    ]
    for load in loads:
        load.start()
    held[0, 0:tokens] = rows_ref[...]
    metas[0, 0:8] = meta_ref[...]
    pl.semaphore_wait(barrier, peers - 1 + len(near))

    def place(k, way):
        if isinstance(k, int) and k == half:
            return 0, slice(tokens, 2 * tokens)
        return k, slice(0, tokens) if way == 0 else slice(tokens, 2 * tokens)

    def columns(c):
        return slice(c * cut, (c + 1) * cut)

    def gather_copy(k, way, c):
        if isinstance(k, int) and k == 1:
            source = rows_ref.at[:, columns(c)]
        else:
            at, span = place(k - 1, way)
            source = held.at[at, span, columns(c)]
        at, span = place(k, way)
        return pltpu.make_async_remote_copy(
            source, held.at[at, span, columns(c)],
            ag_send.at[way, k, c], ag_recv.at[way, k, c],
            device_id={"ep_0": beside[way]}, device_id_type=MESH,
        )

    def meta_place(k, way):
        if isinstance(k, int) and k == half:
            return 0, slice(8, 16)
        return k, slice(0, 8) if way == 0 else slice(8, 16)

    def meta_copy(k, way):
        if isinstance(k, int) and k == 1:
            source = meta_ref
        else:
            at, span = meta_place(k - 1, way)
            source = metas.at[at, span]
        at, span = meta_place(k, way)
        return pltpu.make_async_remote_copy(
            source, metas.at[at, span], meta_send.at[way, k], meta_recv.at[way, k],
            device_id={"ep_0": beside[way]}, device_id_type=MESH,
        )

    def block(number):
        return pl.ds(pl.multiple_of(number * slots, slots), slots)

    def out_copy(k, i):
        number, there = peer(i)
        return pltpu.make_async_remote_copy(
            outgoing.at[k, block(number)], arrived.at[k, block(me)],
            out_send.at[k, i], out_recv.at[k, i], device_id=there, device_id_type=MESH,
        )

    def out_landed(k, i):
        number, there = peer(peers - i)
        return pltpu.make_async_remote_copy(
            outgoing.at[k, block(number)], arrived.at[k, block(number)],
            out_send.at[k, i], out_recv.at[k, i], device_id=there, device_id_type=MESH,
        )

    def back_copy(k, i):
        number, there = peer(i)
        return pltpu.make_async_remote_copy(
            results.at[k, block(number)], back.at[k, block(me)],
            back_send.at[k, i], back_recv.at[k, i], device_id=there, device_id_type=MESH,
        )

    def back_landed(k, i):
        number, there = peer(peers - i)
        return pltpu.make_async_remote_copy(
            results.at[k, block(number)], back.at[k, block(number)],
            back_send.at[k, i], back_recv.at[k, i], device_id=there, device_id_type=MESH,
        )

    experts = (z * peers + lax.broadcasted_iota(jnp.int32, (peers, tokens), 0)).astype(jnp.float32)
    earlier = (
        lax.broadcasted_iota(jnp.int32, (tokens, tokens), 0)
        < lax.broadcasted_iota(jnp.int32, (tokens, tokens), 1)
    ).astype(jnp.bfloat16)
    line = lax.broadcasted_iota(jnp.int32, (peers * slots, tokens), 0)
    slot_of = lax.rem(line, cap).astype(jnp.float32)
    side_of = lax.rem(line // cap, 2)

    def dispatch(k):
        meta = metas[k]
        chosen, weighted = [], []
        for side in range(2):
            hits = jnp.zeros((peers, tokens), jnp.float32)
            weights = jnp.zeros((peers, tokens), jnp.float32)
            for choice in range(4):
                row = meta[side * 8 + choice : side * 8 + choice + 1]
                weight = meta[side * 8 + 4 + choice : side * 8 + 5 + choice]
                hit = jnp.where(row == experts, 1.0, 0.0)
                hits = hits + hit
                weights = weights + hit * weight
            rank = jnp.dot(
                hits.astype(jnp.bfloat16), earlier, preferred_element_type=jnp.float32
            )
            rank = jnp.where(hits > 0.5, rank, -1.0)
            match = (plane_rows(rank, slots) == slot_of) & (side_of == side)
            chosen.append(jnp.where(match, 1.0, 0.0))
            weighted.append(jnp.where(match, plane_rows(weights, slots), 0.0))
        picks[k] = jnp.concatenate(weighted, axis=1).astype(jnp.bfloat16)
        choose = jnp.concatenate(chosen, axis=1).astype(jnp.bfloat16)
        tile = 512

        @pl.loop(0, width // tile)
        def _(n):
            span = pl.ds(pl.multiple_of(n * tile, tile), tile)
            outgoing[k, :, span] = jnp.dot(
                choose, held[k, :, span], preferred_element_type=jnp.float32
            ).astype(jnp.bfloat16)

        for i in range(1, peers):
            out_copy(k, i).start()
        arrived[k, block(me)] = outgoing[k, block(me)]

    def experts_on(k):
        for i in range(1, peers):
            out_landed(k, i).wait_recv()
        tile = 256

        @pl.loop(0, hidden.shape[1] // tile)
        def _(n):
            span = pl.ds(pl.multiple_of(n * tile, tile), tile)
            gate = jnp.dot(arrived[k], gate_ref[:, span], preferred_element_type=jnp.float32)
            lift = jnp.dot(arrived[k], lift_ref[:, span], preferred_element_type=jnp.float32)
            hidden[:, span] = (gate / (1.0 + jnp.exp(-gate)) * lift).astype(jnp.bfloat16)

        @pl.loop(0, width // tile)
        def _(n):
            span = pl.ds(pl.multiple_of(n * tile, tile), tile)
            results[k, :, span] = jnp.dot(
                hidden[...], drop_ref[:, span], preferred_element_type=jnp.float32
            ).astype(jnp.bfloat16)

        for i in range(1, peers):
            back_copy(k, i).start()
        back[k, block(me)] = results[k, block(me)]

    side_cols = (lax.rem(col + 1, nx), lax.rem(col + nx - 1, nx))
    turn = nx // 2

    def off(k, way):
        return lax.rem(col + k, nx) if way == 0 else lax.rem(col + nx - k, nx)

    def row_block(number):
        return pl.ds(pl.multiple_of(number * tokens, tokens), tokens)

    def spread_copy(which, k, way, c, landed=False):
        source, full = (mix_ref, mix_all) if which == 0 else (rows_ref, exp_all)
        at = row_block(off(k if landed else k - 1, 1 - way))
        return pltpu.make_async_remote_copy(
            source.at[:, columns(c)] if k == 1 else full.at[at, columns(c)],
            full.at[at, columns(c)],
            xg_send.at[which, k, way, c], xg_recv.at[which, k, way, c],
            device_id={"tp": side_cols[way]}, device_id_type=MESH,
        )

    def spread_start(which):
        for c in range(2):
            for way in range(2):
                spread_copy(which, 1, way, c).start()

    def spread_turn(which):
        for c in range(2):
            for way in range(2):
                spread_copy(which, 1, way, c, True).wait_recv()
                if way == c:
                    spread_copy(which, turn, way, c).start()

    def spread_end(which):
        for c in range(2):
            spread_copy(which, turn, c, c, True).wait_recv()

    def spread_sent(which):
        for c in range(2):
            for way in range(2):
                spread_copy(which, 1, way, c).wait_send()
            spread_copy(which, turn, c, c).wait_send()

    def fold_copy(which, k, way, c):
        part, sums_in = (mix_part, mix_sums) if which == 0 else (exp_part, exp_sums)
        return pltpu.make_async_remote_copy(
            part.at[row_block(off(k, way)), columns(c)],
            sums_in.at[way, k - 1, :, columns(c)],
            xr_send.at[which, k, way, c], xr_recv.at[which, k, way, c],
            device_id={"tp": side_cols[way]}, device_id_type=MESH,
        )

    def fold_start(which):
        for c in range(2):
            fold_copy(which, turn, c, c).start()
            fold_copy(which, 1, 1 - c, c).start()

    def fold_turn(which):
        part, sums_in = (mix_part, mix_sums) if which == 0 else (exp_part, exp_sums)
        for c in range(2):
            fold_copy(which, turn, c, c).wait_recv()
            at = row_block(off(1, c))
            part[at, columns(c)] = (
                part[at, columns(c)].astype(jnp.float32)
                + sums_in[c, 1, :, columns(c)].astype(jnp.float32)
            ).astype(jnp.bfloat16)
            fold_copy(which, 1, c, c).start()

    def fold_end(which, c):
        part, sums_in = (mix_part, mix_sums) if which == 0 else (exp_part, exp_sums)
        total = part[row_block(col), columns(c)].astype(jnp.float32)
        for way in range(2):
            fold_copy(which, 1, way, c).wait_recv()
            total = total + sums_in[way, 0, :, columns(c)].astype(jnp.float32)
        return total

    def fold_sent(which):
        for c in range(2):
            for way in range(2):
                fold_copy(which, 1, way, c).wait_send()
            fold_copy(which, turn, c, c).wait_send()

    keys = q_rows.shape[1]
    values = v_rows.shape[1]
    dv = values // (keys // DK)
    lane_head = lax.broadcasted_iota(jnp.int32, (1, keys), 1) // DK
    head_masks = [jnp.where(lane_head == h, 1.0, 0.0) for h in range(2)]

    def project():
        @pl.loop(0, mix_all.shape[0] // (2 * tokens))
        def _(n):
            span = pl.ds(pl.multiple_of(n * 2 * tokens, 2 * tokens), 2 * tokens)
            rows = mix_all[span]
            f32 = jnp.float32
            query = jnp.dot(rows, query_ref[...], preferred_element_type=f32)
            q_rows[span] = query.astype(jnp.bfloat16)
            key = jnp.dot(rows, key_ref[...], preferred_element_type=f32)
            k_rows[span] = key.astype(jnp.bfloat16)
            value = jnp.dot(rows, value_ref[...], preferred_element_type=f32)
            v_rows[span] = value.astype(jnp.bfloat16)
            low = jnp.dot(rows, low_ref[...], preferred_element_type=f32).astype(jnp.bfloat16)
            logit = jnp.dot(low, decay_ref[...], preferred_element_type=f32) + bias_ref[...]
            soft = jnp.minimum(logit, 0.0) - jnp.log1p(jnp.exp(-jnp.abs(logit)))
            decays[span] = soft * (1.0 / gate_norm) + shift_ref[span]

        state[...] = jnp.zeros_like(state)
        before[...] = jnp.zeros_like(before)

    def scan_blocks(start, stop):
        low_tri = jnp.where(
            lax.broadcasted_iota(jnp.int32, (BLOCK, BLOCK), 0)
            >= lax.broadcasted_iota(jnp.int32, (BLOCK, BLOCK), 1),
            1.0,
            0.0,
        )
        causal = jnp.concatenate([low_tri, low_tri], axis=0)
        head_mask = jnp.concatenate(
            [jnp.broadcast_to(m, (dv, keys)) for m in head_masks], axis=0
        )

        @pl.loop(start, stop)
        def _(n):
            span = pl.ds(pl.multiple_of(n * BLOCK, BLOCK), BLOCK)
            within = jnp.dot(
                low_tri, decays[span], precision=highest, preferred_element_type=jnp.float32
            )
            total = within[BLOCK - 1 : BLOCK]
            query = q_rows[span].astype(jnp.float32) * DK ** (-0.5)
            key = k_rows[span].astype(jnp.float32)
            value = v_rows[span]
            scaled = query * jnp.exp(within)
            scaled_key = (key * jnp.exp(-within)).astype(jnp.bfloat16)
            kept_key = (key * jnp.exp(total - within)).astype(jnp.bfloat16)
            both = jnp.concatenate([scaled * m for m in head_masks], axis=0).astype(jnp.bfloat16)
            scores = lax.dot_general(
                both, scaled_key, (((1,), (1,)), ((), ())), preferred_element_type=jnp.float32
            )
            scores = jnp.where(causal > 0.5, scores, 0.0).astype(jnp.bfloat16)
            mixed = jnp.dot(scores, value, preferred_element_type=jnp.float32)
            mixed = jnp.concatenate([mixed[:BLOCK, :dv], mixed[BLOCK:, dv:]], axis=1)
            mixed = mixed + lax.dot_general(
                scaled.astype(jnp.bfloat16), state[...].astype(jnp.bfloat16),
                (((1,), (1,)), ((), ())), preferred_element_type=jnp.float32,
            )
            inner[span] = mixed
            added = lax.dot_general(
                value, kept_key, (((0,), (0,)), ((), ())), preferred_element_type=jnp.float32
            )
            state[...] = jnp.exp(total) * state[...] + added * head_mask
            carried[span] = (query * jnp.exp(within + before[0:1])).astype(jnp.bfloat16)
            before[...] = before[...] + total

    mate = {"ep_1": nc - 1 - core}

    def mate_copy(part):
        source, target = (
            (chip_state, mate_state), (chip_total, mate_total),
            (scan_out.at[len(reaches) + 1], entering.at[pl.ds(pl.multiple_of(core * (dv // 2), dv // 2), dv // 2)]),
        )[part]
        return pltpu.make_async_remote_copy(
            source, target, mate_send.at[part], mate_recv.at[part],
            device_id=mate, device_id_type=MESH,
        )

    def mate_half_landed():
        other = nc - 1 - core
        return pltpu.make_async_remote_copy(
            scan_out.at[len(reaches) + 1],
            entering.at[pl.ds(pl.multiple_of(other * (dv // 2), dv // 2), dv // 2)],
            mate_send.at[2], mate_recv.at[2], device_id=mate, device_id_type=MESH,
        )

    def states_out():
        packed = state[0:dv] * head_masks[0] + state[dv:] * head_masks[1]
        chip_state[...] = packed.astype(jnp.bfloat16)
        chip_total[...] = before[...]
        mate_copy(0).start()
        mate_copy(1).start()

    def scan_copies(step):
        there = {"ep_0": lax.rem(z + (1 if step == 0 else reaches[step - 1]), nz)}
        return [
            pltpu.make_async_remote_copy(
                a.at[step], b.at[step], scan_send.at[step, n], scan_recv.at[step, n],
                device_id=there, device_id_type=MESH,
            )
            for n, (a, b) in enumerate(
                ((scan_out, scan_in), (scan_total_out, scan_total_in))
            )
        ]

    def scan_start(step):
        scan_out[step] = prefix[...].astype(jnp.bfloat16)
        scan_total_out[step] = prefix_total[...]
        for copy in scan_copies(step):
            copy.start()

    def scan_open():
        mate_copy(0).wait_recv()
        mate_copy(1).wait_recv()
        early = core == 0
        own, own_total = chip_state[...].astype(jnp.float32), chip_total[...]
        far, far_total = mate_state[...].astype(jnp.float32), mate_total[...]
        later_total = jnp.where(early, far_total[0:1], own_total[0:1])
        joined = jnp.exp(later_total) * jnp.where(early, own, far) + jnp.where(early, far, own)
        prefix[...] = jnp.where(early, joined[: dv // 2], joined[dv // 2 :])
        prefix_total[...] = own_total + far_total
        scan_start(0)

    def scan_step(step):
        for copy in scan_copies(step):
            copy.wait_recv()
        came = scan_in[step].astype(jnp.float32)
        came_total = scan_total_in[step]
        if step == 0:
            valid = z >= 1
            prefix[...] = jnp.where(valid, came, 0.0)
            prefix_total[...] = jnp.where(valid, came_total, 0.0)
        else:
            valid = z >= reaches[step - 1]
            joined = jnp.exp(prefix_total[0:1]) * came + prefix[...]
            prefix[...] = jnp.where(valid, joined, prefix[...])
            prefix_total[...] = jnp.where(
                valid, prefix_total[...] + came_total, prefix_total[...]
            )
        if step < len(reaches):
            scan_start(step + 1)
        else:
            mine = prefix[...].astype(jnp.bfloat16)
            scan_out[step + 1] = mine
            entering[pl.ds(pl.multiple_of(core * (dv // 2), dv // 2), dv // 2)] = mine
            mate_copy(2).start()

    def finish_mixer():
        mate_half_landed().wait_recv()
        come = entering[...].astype(jnp.float32)
        behind = jnp.exp(mate_total[0:1]) * come + mate_state[...].astype(jnp.float32)
        come = jnp.where(core == 0, come, behind)
        spread_sent(0)
        wide = jnp.concatenate([come * m for m in head_masks], axis=0).astype(jnp.bfloat16)

        @pl.loop(0, nx)
        def _(b):
            span = row_block(b)
            attended = inner[span] + lax.dot_general(
                carried[span], wide, (((1,), (1,)), ((), ())), preferred_element_type=jnp.float32
            )
            heads = []
            for h in range(2):
                one = attended[:, h * dv : (h + 1) * dv]
                inverse = lax.rsqrt(jnp.mean(one * one, axis=-1, keepdims=True) + epsilon)
                heads.append((one * inverse * gain_ref[...]).astype(jnp.bfloat16))
            mix_part[span] = jnp.dot(
                jnp.concatenate(heads, axis=1), mixout_ref[...], preferred_element_type=jnp.float32
            ).astype(jnp.bfloat16)

        fold_start(0)

    def shared():
        @pl.loop(0, nx // 2)
        def _(n):
            span = pl.ds(pl.multiple_of(n * 2 * tokens, 2 * tokens), 2 * tokens)
            rows = exp_all[span]
            gate = jnp.dot(rows, sgate_ref[...], preferred_element_type=jnp.float32)
            lift = jnp.dot(rows, slift_ref[...], preferred_element_type=jnp.float32)
            unit = (gate / (1.0 + jnp.exp(-gate)) * lift).astype(jnp.bfloat16)
            exp_part[span] = jnp.dot(
                unit, sdrop_ref[...], preferred_element_type=jnp.float32
            ).astype(jnp.bfloat16)

        fold_start(1)

    mix_all[row_block(col)] = mix_ref[...]
    exp_all[row_block(col)] = rows_ref[...]
    spread_start(0)
    for c in range(2):
        for way in range(2):
            gather_copy(1, way, c).start()
    for way in range(2):
        meta_copy(1, way).start()

    def step(k):
        for c in range(2):
            for way in range(2):
                gather_copy(k, way, c).wait_recv()
                gather_copy(k + 1, way, c).start()
        for way in range(2):
            meta_copy(k, way).wait_recv()
            meta_copy(k + 1, way).start()
        dispatch(k)

    for c in range(2):
        for way in range(2):
            gather_copy(1, way, c).wait_recv()
            gather_copy(2, way, c).start()
    for way in range(2):
        meta_copy(1, way).wait_recv()
        meta_copy(2, way).start()
    dispatch(1)
    for load in loads:
        load.wait()
    spread_turn(0)
    blocks = mix_all.shape[0] // BLOCK

    @pl.loop(2, half - 1)
    def _(k):
        step(k)

        @pl.when(k == 2)
        def _():
            spread_end(0)
            project()
            spread_start(1)

        experts_on(k - 1)

        @pl.when(k == 3)
        def _():
            spread_turn(1)

        @pl.when((k == 3) | (k == 4))
        def _():
            scan_blocks((k - 3) * (blocks // 2), (k - 2) * (blocks // 2))

        @pl.when(k == 4)
        def _():
            states_out()

        @pl.when(k == 5)
        def _():
            scan_open()
            spread_end(1)
            shared()

        @pl.when(k == 6)
        def _():
            scan_step(0)
            fold_turn(1)

    last = half - 1
    for c in range(2):
        for way in range(2):
            gather_copy(last, way, c).wait_recv()
            if way == c:
                gather_copy(half, way, c).start()
    for way in range(2):
        meta_copy(last, way).wait_recv()
    meta_copy(half, 0).start()
    dispatch(last)
    experts_on(last - 1)
    scan_step(1)
    for c in range(2):
        gather_copy(half, c, c).wait_recv()
    meta_copy(half, 0).wait_recv()
    dispatch(0)
    experts_on(last)
    scan_step(2)
    experts_on(0)

    def combined(k, span):
        return lax.dot_general(
            picks[k], back[k, :, span], (((0,), (0,)), ((), ())),
            preferred_element_type=jnp.float32,
        )

    def returned(k):
        for i in range(1, peers):
            back_landed(k, i).wait_recv()

    def sum_copy(k, way, c):
        if isinstance(k, int) and k == half:
            source = first.at[:, columns(c)]
        else:
            source = sums.at[way, k, :, columns(c)]
        return pltpu.make_async_remote_copy(
            source, sums.at[way, k - 1, :, columns(c)],
            rs_send.at[way, k, c], rs_recv.at[way, k, c],
            device_id={"ep_0": beside[way]}, device_id_type=MESH,
        )

    returned(0)
    for c in range(2):
        both = combined(0, columns(c))
        own_sum[:, columns(c)] = both[0:tokens]
        first[:, columns(c)] = both[tokens:].astype(jnp.bfloat16)
        sum_copy(half, c, c).start()

    def pass_on(k, c, landed):
        both = combined(k, columns(c))
        for way in range(2):
            part = both[tokens:] if way == 0 else both[0:tokens]
            if landed(way, c):
                sum_copy(k + 1, way, c).wait_recv()
                part = part + sums[way, k, :, columns(c)].astype(jnp.float32)
            sums[way, k, :, columns(c)] = part.astype(jnp.bfloat16)
            sum_copy(k, way, c).start()

    returned(last)
    for c in range(2):
        pass_on(last, c, lambda way, c: way == c)
    scan_step(3)

    @pl.loop(1, last)
    def _(n):
        k = last - n
        returned(k)
        for c in range(2):
            pass_on(k, c, lambda way, c: True)

        @pl.when(n == 1)
        def _():
            scan_step(4)

        @pl.when(n == 2)
        def _():
            finish_mixer()

        @pl.when(n == 4)
        def _():
            fold_turn(0)

    for c in range(2):
        mixed_ref[:, columns(c)] = fold_end(0, c).astype(jnp.bfloat16)
        own_sum[:, columns(c)] += fold_end(1, c)

    for c in range(2):
        total = own_sum[:, columns(c)]
        for way in range(2):
            sum_copy(1, way, c).wait_recv()
            total = total + sums[way, 0, :, columns(c)].astype(jnp.float32)
        out_ref[:, columns(c)] = total.astype(jnp.bfloat16)

    spread_sent(1)
    for which in range(2):
        fold_sent(which)
    for part in range(3):
        mate_copy(part).wait_send()
    for number in range(len(reaches) + 1):
        for copy in scan_copies(number):
            copy.wait_send()

    for c in range(2):
        for way in range(2):
            gather_copy(1, way, c).wait_send()
            sum_copy(1, way, c).wait_send()
            if way == c:
                gather_copy(half, way, c).wait_send()
                sum_copy(half, way, c).wait_send()
    for way in range(2):
        meta_copy(1, way).wait_send()
    meta_copy(half, 0).wait_send()

    @pl.loop(2, half)
    def _(k):
        for way in range(2):
            for c in range(2):
                gather_copy(k, way, c).wait_send()
                sum_copy(k, way, c).wait_send()
            meta_copy(k, way).wait_send()

    @pl.loop(0, half)
    def _(k):
        for i in range(1, peers):
            out_copy(k, i).wait_send()
            back_copy(k, i).wait_send()


def fused(
    mesh_sizes, mix_normed, rows, ids, weights, shift, decay_cols, bias_cols, head_gain,
    w_gate, w_lift, w_drop, w_query, w_key, w_value, w_lowrank, w_output,
    shared_gate, shared_lift, shared_drop,
):
    nz, nc, nx = mesh_sizes
    half, peers = nz // 2, nc * nx
    tokens, width = rows.shape
    ff = w_gate.shape[-1]
    cap = 2 * tokens * ids.shape[1] // (nz * peers)
    slots = 2 * cap
    span = nx * tokens
    keys, values = w_query.shape[1], w_value.shape[1]
    dv = values * DK // keys
    scans = len([d for d in (1, 2, 4, 8, 16, 32) if d < nz]) + 1
    meta = jnp.concatenate([ids.T.astype(jnp.float32), weights.T], axis=0)
    vmem, dma = pltpu.VMEM, pltpu.SemaphoreType.DMA
    bf, f32 = jnp.bfloat16, jnp.float32
    whole = pl.BlockSpec(memory_space=pltpu.VMEM)
    anywhere = pl.BlockSpec(memory_space=pl.ANY)
    return pl.pallas_call(
        functools.partial(moe_kernel, nz, nc, nx),
        out_shape=(jax.ShapeDtypeStruct((tokens, width), bf),) * 2,
        in_specs=[whole] * 7 + [anywhere] * 11,
        out_specs=(whole, whole),
        scratch_shapes=[
            vmem((half, 2 * tokens, width), bf),
            vmem((half, 16, tokens), f32),
            vmem((half, peers * slots, 2 * tokens), bf),
            vmem((half, peers * slots, width), bf),
            vmem((half, peers * slots, width), bf),
            vmem((half, peers * slots, width), bf),
            vmem((half, peers * slots, width), bf),
            vmem((2, half, tokens, width), bf),
            vmem((tokens, width), bf),
            vmem((width, ff), bf),
            vmem((width, ff), bf),
            vmem((ff, width), bf),
            vmem((width, keys), bf),
            vmem((width, keys), bf),
            vmem((width, values), bf),
            vmem(w_lowrank.shape, bf),
            vmem((values, width), bf),
            vmem(shared_gate.shape, bf),
            vmem(shared_lift.shape, bf),
            vmem(shared_drop.shape, bf),
            vmem((peers * slots, ff), bf),
            vmem((tokens, width), f32),
            vmem((span, width), bf),
            vmem((span, width), bf),
            vmem((span, width), bf),
            vmem((2, 2, tokens, width), bf),
            vmem((2, 2, tokens, width), bf),
            vmem((span, keys), bf),
            vmem((span, keys), bf),
            vmem((span, values), bf),
            vmem((span, keys), f32),
            vmem((span, values), f32),
            vmem((span, keys), bf),
            vmem((values, keys), f32),
            vmem((8, keys), f32),
            vmem((dv, keys), bf),
            vmem((8, keys), f32),
            vmem((dv, keys), bf),
            vmem((8, keys), f32),
            vmem((dv // 2, keys), f32),
            vmem((8, keys), f32),
            vmem((scans + 1, dv // 2, keys), bf),
            vmem((scans, 8, keys), f32),
            vmem((scans, dv // 2, keys), bf),
            vmem((scans, 8, keys), f32),
            vmem((dv, keys), bf),
            dma((2, half + 1, 2)), dma((2, half + 1, 2)),
            dma((2, half + 1)), dma((2, half + 1)),
            dma((half, peers)), dma((half, peers)),
            dma((half, peers)), dma((half, peers)),
            dma((2, half + 1, 2)), dma((2, half + 1, 2)),
            dma((11,)),
            dma((2, 3, 2, 2)), dma((2, 3, 2, 2)),
            dma((2, 3, 2, 2)), dma((2, 3, 2, 2)),
            dma((3,)), dma((3,)),
            dma((scans, 2)), dma((scans, 2)),
        ],
        compiler_params=pltpu.CompilerParams(
            collective_id=0, has_side_effects=True, vmem_limit_bytes=63 * 1024 * 1024
        ),
        cost_estimate=pl.CostEstimate(
            flops=200_000_000_000, bytes_accessed=16 * 2**20, transcendentals=0
        ),
    )(
        mix_normed, rows, meta, shift, decay_cols, bias_cols, head_gain,
        w_gate[0], w_lift[0], w_drop[0], w_query, w_key, w_value, w_lowrank, w_output,
        shared_gate, shared_lift, shared_drop,
    )


def body(
    mix_rows,
    expert_rows,
    mix_gain,
    ffn_gain,
    w_query,
    w_key,
    w_value,
    w_lowrank,
    w_decay,
    decay_bias,
    decay_shift,
    head_gain,
    w_output,
    route_ids,
    route_weights,
    w_gate,
    w_lift,
    w_drop,
    shared_gate,
    shared_lift,
    shared_drop,
):
    mix_normed = layer_norm(mix_rows, mix_gain)
    local_heads = w_query.shape[1] // DK
    key_cols = local_heads * DK
    column = lax.axis_index("tp") * key_cols
    decay_cols = lax.dynamic_slice_in_dim(w_decay, column, key_cols, 1)
    bias_cols = lax.dynamic_slice_in_dim(decay_bias, column, key_cols, 0)
    expert_normed = layer_norm(expert_rows, ffn_gain)
    shift = jnp.repeat(jnp.transpose(decay_shift), DK, axis=1)
    sizes = (lax.axis_size("ep_0"), lax.axis_size("ep_1"), lax.axis_size("tp"))
    return fused(
        sizes, mix_normed, expert_normed, route_ids, route_weights, shift, decay_cols,
        bias_cols[None], head_gain[None], w_gate, w_lift, w_drop, w_query, w_key, w_value,
        w_lowrank, w_output, shared_gate, shared_lift, shared_drop,
    )


def solution(mesh):
    finer = Mesh(
        mesh.devices.reshape(mesh.shape["grp"], 16, 2, mesh.shape["tp"]),
        ("grp", "ep_0", "ep_1", "tp"),
    )
    in_specs = (
        P(GRP_EP_TP, None),
        P(GRP_EP_TP, None),
        P(),
        P(),
        P(None, "tp"),
        P(None, "tp"),
        P(None, "tp"),
        P(),
        P(),
        P(),
        P("tp", GRP_EP),
        P(),
        P("tp", None),
        P(GRP_EP_TP, None),
        P(GRP_EP_TP, None),
        P(EP_TP, None, None),
        P(EP_TP, None, None),
        P(EP_TP, None, None),
        P(None, "tp"),
        P(None, "tp"),
        P("tp", None),
    )
    out_specs = (P(GRP_EP_TP, None), P(GRP_EP_TP, None))
    return jax.shard_map(body, mesh=finer, in_specs=in_specs, out_specs=out_specs, check_vma=False)
```

```python
import functools

import jax
import jax.numpy as jnp
from jax import lax
from jax.experimental import pallas as pl
from jax.experimental.pallas import tpu as pltpu
from jax.sharding import Mesh
from jax.sharding import PartitionSpec as P

DK = 64
DV = 128
BLOCK = 64
EP = ("ep_0", "ep_1")
EP_TP = ("ep_0", "ep_1", "tp")
GRP_EP_TP = ("grp", "ep_0", "ep_1", "tp")
GRP_EP = ("grp", "ep_0", "ep_1")


epsilon = 1e-05
gate_norm = 16.0
highest = lax.Precision.HIGHEST


def layer_norm(source, gain):
    values = source.astype(jnp.float32)
    center = values - jnp.mean(values, axis=-1, keepdims=True)
    inverse = lax.rsqrt(jnp.mean(center * center, axis=-1, keepdims=True) + epsilon)
    return (center * inverse * gain).astype(jnp.bfloat16)


MESH = pl.DeviceIdType.MESH


def plane_rows(values, width):
    return jnp.concatenate(
        [jnp.broadcast_to(values[j : j + 1], (width, values.shape[1])) for j in range(len(values))],
        axis=0,
    )


def moe_kernel(
    nz, nc, nx,
    mix_ref, rows_ref, mix_gain_ref, ffn_gain_ref, meta_ref, shift_ref, decay_ref, bias_ref,
    gain_ref,
    gate_hbm, lift_hbm, drop_hbm, query_hbm, key_hbm, value_hbm, low_hbm, mixout_hbm,
    sgate_hbm, slift_hbm, sdrop_hbm,
    mixed_ref, out_ref,
    held, metas, picks, outgoing, arrived, results, back, sums, first,
    gate_ref, lift_ref, drop_ref, query_ref, key_ref, value_ref, low_ref, mixout_ref,
    sgate_ref, slift_ref, sdrop_ref, hidden, own_sum,
    mix_all, exp_all, exp_part, mix_sums, exp_sums,
    q_rows, k_rows, v_rows, decays, inner, carried, state, before,
    chip_state, chip_total, mate_state, mate_total, prefix, prefix_total,
    scan_out, scan_total_out, scan_in, scan_total_in, entering,
    ag_send, ag_recv, meta_send, meta_recv, out_send, out_recv, back_send, back_recv,
    rs_send, rs_recv, load_sem,
    xg_send, xg_recv, xr_send, xr_recv, mate_send, mate_recv, scan_send, scan_recv,
):
    half = nz // 2
    peers = nc * nx
    mix_part = mix_all
    z = lax.axis_index("ep_0")
    core = lax.axis_index("ep_1")
    col = lax.axis_index("tp")
    me = core * nx + col
    tokens, width = rows_ref.shape
    cut = width // 2
    slots = arrived.shape[1] // peers
    cap = slots // 2
    right, left = lax.rem(z + 1, nz), lax.rem(z + nz - 1, nz)
    beside = (right, left)

    def peer(i):
        number = lax.rem(me + i, peers)
        return number, {"ep_1": number // nx, "tp": lax.rem(number, nx)}

    barrier = pltpu.get_barrier_semaphore()
    reaches = [d for d in (1, 2, 4, 8, 16, 32) if d < nz]
    near = sorted({d % nz for d in reaches} | {-d % nz for d in reaches})
    for d in near:
        there = {"ep_0": lax.rem(z + d, nz)}
        pl.semaphore_signal(barrier, inc=1, device_id=there, device_id_type=MESH)
    for i in range(1, peers):
        pl.semaphore_signal(barrier, inc=1, device_id=peer(i)[1], device_id_type=MESH)
    loads = [
        pltpu.make_async_copy(a, b, load_sem.at[k])
        for k, (a, b) in enumerate(
            (
                (query_hbm, query_ref), (key_hbm, key_ref), (value_hbm, value_ref),
                (low_hbm, low_ref), (gate_hbm, gate_ref), (lift_hbm, lift_ref),
                (drop_hbm, drop_ref), (sgate_hbm, sgate_ref), (slift_hbm, slift_ref),
                (sdrop_hbm, sdrop_ref), (mixout_hbm, mixout_ref),
            )
        )
    ]
    for load in loads:
        load.start()
    metas[0, 0:8] = meta_ref[...]
    own = pl.multiple_of(col * tokens, tokens)
    rows_at_once = 16

    @pl.loop(0, tokens // rows_at_once)
    def _(n):
        start = pl.multiple_of(n * rows_at_once, rows_at_once)
        span, there = pl.ds(start, rows_at_once), pl.ds(own + start, rows_at_once)
        mix_all[there] = layer_norm(mix_ref[span], mix_gain_ref[...])
        normed = layer_norm(rows_ref[span], ffn_gain_ref[...])
        held[0, span] = normed
        exp_all[there] = normed

    pl.semaphore_wait(barrier, peers - 1 + len(near))

    def place(k, way):
        if isinstance(k, int) and k == half:
            return 0, slice(tokens, 2 * tokens)
        return k, slice(0, tokens) if way == 0 else slice(tokens, 2 * tokens)

    def columns(c):
        return slice(c * cut, (c + 1) * cut)

    def gather_copy(k, way, c):
        if isinstance(k, int) and k == 1:
            source = held.at[0, slice(0, tokens), columns(c)]
        else:
            at, span = place(k - 1, way)
            source = held.at[at, span, columns(c)]
        at, span = place(k, way)
        return pltpu.make_async_remote_copy(
            source, held.at[at, span, columns(c)],
            ag_send.at[way, k, c], ag_recv.at[way, k, c],
            device_id={"ep_0": beside[way]}, device_id_type=MESH,
        )

    def meta_place(k, way):
        if isinstance(k, int) and k == half:
            return 0, slice(8, 16)
        return k, slice(0, 8) if way == 0 else slice(8, 16)

    def meta_copy(k, way):
        if isinstance(k, int) and k == 1:
            source = meta_ref
        else:
            at, span = meta_place(k - 1, way)
            source = metas.at[at, span]
        at, span = meta_place(k, way)
        return pltpu.make_async_remote_copy(
            source, metas.at[at, span], meta_send.at[way, k], meta_recv.at[way, k],
            device_id={"ep_0": beside[way]}, device_id_type=MESH,
        )

    def block(number):
        return pl.ds(pl.multiple_of(number * slots, slots), slots)

    def out_copy(k, i):
        number, there = peer(i)
        return pltpu.make_async_remote_copy(
            outgoing.at[k, block(number)], arrived.at[k, block(me)],
            out_send.at[k, i], out_recv.at[k, i], device_id=there, device_id_type=MESH,
        )

    def out_landed(k, i):
        number, there = peer(peers - i)
        return pltpu.make_async_remote_copy(
            outgoing.at[k, block(number)], arrived.at[k, block(number)],
            out_send.at[k, i], out_recv.at[k, i], device_id=there, device_id_type=MESH,
        )

    def back_copy(k, i):
        number, there = peer(i)
        return pltpu.make_async_remote_copy(
            results.at[k, block(number)], back.at[k, block(me)],
            back_send.at[k, i], back_recv.at[k, i], device_id=there, device_id_type=MESH,
        )

    def back_landed(k, i):
        number, there = peer(peers - i)
        return pltpu.make_async_remote_copy(
            results.at[k, block(number)], back.at[k, block(number)],
            back_send.at[k, i], back_recv.at[k, i], device_id=there, device_id_type=MESH,
        )

    experts = (z * peers + lax.broadcasted_iota(jnp.int32, (peers, tokens), 0)).astype(jnp.float32)
    earlier = (
        lax.broadcasted_iota(jnp.int32, (tokens, tokens), 0)
        < lax.broadcasted_iota(jnp.int32, (tokens, tokens), 1)
    ).astype(jnp.bfloat16)
    line = lax.broadcasted_iota(jnp.int32, (peers * slots, tokens), 0)
    slot_of = lax.rem(line, cap).astype(jnp.float32)
    side_of = lax.rem(line // cap, 2)

    def dispatch(k):
        meta = metas[k]
        chosen, weighted = [], []
        for side in range(2):
            hits = jnp.zeros((peers, tokens), jnp.float32)
            weights = jnp.zeros((peers, tokens), jnp.float32)
            for choice in range(4):
                row = meta[side * 8 + choice : side * 8 + choice + 1]
                weight = meta[side * 8 + 4 + choice : side * 8 + 5 + choice]
                hit = jnp.where(row == experts, 1.0, 0.0)
                hits = hits + hit
                weights = weights + hit * weight
            rank = jnp.dot(
                hits.astype(jnp.bfloat16), earlier, preferred_element_type=jnp.float32
            )
            rank = jnp.where(hits > 0.5, rank, -1.0)
            match = (plane_rows(rank, slots) == slot_of) & (side_of == side)
            chosen.append(jnp.where(match, 1.0, 0.0))
            weighted.append(jnp.where(match, plane_rows(weights, slots), 0.0))
        picks[k] = jnp.concatenate(weighted, axis=1).astype(jnp.bfloat16)
        choose = jnp.concatenate(chosen, axis=1).astype(jnp.bfloat16)
        tile = 512

        @pl.loop(0, width // tile)
        def _(n):
            span = pl.ds(pl.multiple_of(n * tile, tile), tile)
            outgoing[k, :, span] = jnp.dot(
                choose, held[k, :, span], preferred_element_type=jnp.float32
            ).astype(jnp.bfloat16)

        for i in range(1, peers):
            out_copy(k, i).start()
        arrived[k, block(me)] = outgoing[k, block(me)]

    def experts_on(k):
        for i in range(1, peers):
            out_landed(k, i).wait_recv()
        tile = 256

        @pl.loop(0, hidden.shape[1] // tile)
        def _(n):
            span = pl.ds(pl.multiple_of(n * tile, tile), tile)
            gate = jnp.dot(arrived[k], gate_ref[:, span], preferred_element_type=jnp.float32)
            lift = jnp.dot(arrived[k], lift_ref[:, span], preferred_element_type=jnp.float32)
            hidden[:, span] = (gate / (1.0 + jnp.exp(-gate)) * lift).astype(jnp.bfloat16)

        @pl.loop(0, width // tile)
        def _(n):
            span = pl.ds(pl.multiple_of(n * tile, tile), tile)
            results[k, :, span] = jnp.dot(
                hidden[...], drop_ref[:, span], preferred_element_type=jnp.float32
            ).astype(jnp.bfloat16)

        back[k, block(me)] = results[k, block(me)]

    def back_start(k):
        for i in range(1, peers):
            back_copy(k, i).start()

    side_cols = (lax.rem(col + 1, nx), lax.rem(col + nx - 1, nx))
    turn = nx // 2

    def off(k, way):
        return lax.rem(col + k, nx) if way == 0 else lax.rem(col + nx - k, nx)

    def row_block(number):
        return pl.ds(pl.multiple_of(number * tokens, tokens), tokens)

    def spread_copy(which, k, way, c, landed=False):
        full = mix_all if which == 0 else exp_all
        at = row_block(off(k if landed else k - 1, 1 - way))
        return pltpu.make_async_remote_copy(
            full.at[at, columns(c)], full.at[at, columns(c)],
            xg_send.at[which, k, way, c], xg_recv.at[which, k, way, c],
            device_id={"tp": side_cols[way]}, device_id_type=MESH,
        )

    def spread_start(which):
        for c in range(2):
            for way in range(2):
                spread_copy(which, 1, way, c).start()

    def spread_turn(which):
        for c in range(2):
            for way in range(2):
                spread_copy(which, 1, way, c, True).wait_recv()
                if way == c:
                    spread_copy(which, turn, way, c).start()

    def spread_end(which):
        for c in range(2):
            spread_copy(which, turn, c, c, True).wait_recv()

    def spread_sent(which):
        for c in range(2):
            for way in range(2):
                spread_copy(which, 1, way, c).wait_send()
            spread_copy(which, turn, c, c).wait_send()

    def fold_copy(which, k, way, c):
        part, sums_in = (mix_part, mix_sums) if which == 0 else (exp_part, exp_sums)
        return pltpu.make_async_remote_copy(
            part.at[row_block(off(k, way)), columns(c)],
            sums_in.at[way, k - 1, :, columns(c)],
            xr_send.at[which, k, way, c], xr_recv.at[which, k, way, c],
            device_id={"tp": side_cols[way]}, device_id_type=MESH,
        )

    def fold_start(which):
        for c in range(2):
            fold_copy(which, turn, c, c).start()
            fold_copy(which, 1, 1 - c, c).start()

    def fold_turn(which):
        part, sums_in = (mix_part, mix_sums) if which == 0 else (exp_part, exp_sums)
        for c in range(2):
            fold_copy(which, turn, c, c).wait_recv()
            at = row_block(off(1, c))
            part[at, columns(c)] = (
                part[at, columns(c)].astype(jnp.float32)
                + sums_in[c, 1, :, columns(c)].astype(jnp.float32)
            ).astype(jnp.bfloat16)
            fold_copy(which, 1, c, c).start()

    def fold_end(which, c):
        part, sums_in = (mix_part, mix_sums) if which == 0 else (exp_part, exp_sums)
        total = part[row_block(col), columns(c)].astype(jnp.float32)
        for way in range(2):
            fold_copy(which, 1, way, c).wait_recv()
            total = total + sums_in[way, 0, :, columns(c)].astype(jnp.float32)
        return total

    def fold_sent(which):
        for c in range(2):
            for way in range(2):
                fold_copy(which, 1, way, c).wait_send()
            fold_copy(which, turn, c, c).wait_send()

    keys = q_rows.shape[1]
    values = v_rows.shape[1]
    dv = values // (keys // DK)
    lane_head = lax.broadcasted_iota(jnp.int32, (1, keys), 1) // DK
    head_masks = [jnp.where(lane_head == h, 1.0, 0.0) for h in range(2)]

    lanes = pl.ds(pl.multiple_of(col * keys, keys), keys)

    def project():
        @pl.loop(0, mix_all.shape[0] // (2 * tokens))
        def _(n):
            span = pl.ds(pl.multiple_of(n * 2 * tokens, 2 * tokens), 2 * tokens)
            rows = mix_all[span]
            f32 = jnp.float32
            query = jnp.dot(rows, query_ref[...], preferred_element_type=f32)
            q_rows[span] = query.astype(jnp.bfloat16)
            key = jnp.dot(rows, key_ref[...], preferred_element_type=f32)
            k_rows[span] = key.astype(jnp.bfloat16)
            value = jnp.dot(rows, value_ref[...], preferred_element_type=f32)
            v_rows[span] = value.astype(jnp.bfloat16)
            low = lax.dot_general(
                rows, low_ref[...], (((1,), (1,)), ((), ())), preferred_element_type=f32
            ).astype(jnp.bfloat16)
            logit = jnp.dot(low, decay_ref[:, lanes], preferred_element_type=f32) + bias_ref[:, lanes]
            soft = jnp.minimum(logit, 0.0) - jnp.log1p(jnp.exp(-jnp.abs(logit)))
            moved = lax.dot_general(
                shift_ref[:, span], jnp.concatenate(head_masks, axis=0), (((0,), (0,)), ((), ())),
                precision=highest, preferred_element_type=f32,
            )
            decays[span] = soft * (1.0 / gate_norm) + moved

        state[...] = jnp.zeros_like(state)
        before[...] = jnp.zeros_like(before)

    def scan_blocks(start, stop):
        low_tri = jnp.where(
            lax.broadcasted_iota(jnp.int32, (BLOCK, BLOCK), 0)
            >= lax.broadcasted_iota(jnp.int32, (BLOCK, BLOCK), 1),
            1.0,
            0.0,
        )
        causal = jnp.concatenate([low_tri, low_tri], axis=0)
        head_mask = jnp.concatenate(
            [jnp.broadcast_to(m, (dv, keys)) for m in head_masks], axis=0
        )

        @pl.loop(start, stop)
        def _(n):
            span = pl.ds(pl.multiple_of(n * BLOCK, BLOCK), BLOCK)
            within = jnp.dot(
                low_tri, decays[span], precision=highest, preferred_element_type=jnp.float32
            )
            total = within[BLOCK - 1 : BLOCK]
            query = q_rows[span].astype(jnp.float32) * DK ** (-0.5)
            key = k_rows[span].astype(jnp.float32)
            value = v_rows[span]
            scaled = query * jnp.exp(within)
            scaled_key = (key * jnp.exp(-within)).astype(jnp.bfloat16)
            kept_key = (key * jnp.exp(total - within)).astype(jnp.bfloat16)
            both = jnp.concatenate([scaled * m for m in head_masks], axis=0).astype(jnp.bfloat16)
            scores = lax.dot_general(
                both, scaled_key, (((1,), (1,)), ((), ())), preferred_element_type=jnp.float32
            )
            scores = jnp.where(causal > 0.5, scores, 0.0).astype(jnp.bfloat16)
            mixed = jnp.dot(scores, value, preferred_element_type=jnp.float32)
            mixed = jnp.concatenate([mixed[:BLOCK, :dv], mixed[BLOCK:, dv:]], axis=1)
            mixed = mixed + lax.dot_general(
                scaled.astype(jnp.bfloat16), state[...].astype(jnp.bfloat16),
                (((1,), (1,)), ((), ())), preferred_element_type=jnp.float32,
            )
            inner[span] = mixed
            added = lax.dot_general(
                value, kept_key, (((0,), (0,)), ((), ())), preferred_element_type=jnp.float32
            )
            state[...] = jnp.exp(total) * state[...] + added * head_mask
            carried[span] = (query * jnp.exp(within + before[0:1])).astype(jnp.bfloat16)
            before[...] = before[...] + total

    mate = {"ep_1": nc - 1 - core}

    def mate_copy(part):
        source, target = (
            (chip_state, mate_state), (chip_total, mate_total),
            (scan_out.at[len(reaches) + 1], entering.at[pl.ds(pl.multiple_of(core * (dv // 2), dv // 2), dv // 2)]),
        )[part]
        return pltpu.make_async_remote_copy(
            source, target, mate_send.at[part], mate_recv.at[part],
            device_id=mate, device_id_type=MESH,
        )

    def mate_half_landed():
        other = nc - 1 - core
        return pltpu.make_async_remote_copy(
            scan_out.at[len(reaches) + 1],
            entering.at[pl.ds(pl.multiple_of(other * (dv // 2), dv // 2), dv // 2)],
            mate_send.at[2], mate_recv.at[2], device_id=mate, device_id_type=MESH,
        )

    def states_out():
        packed = state[0:dv] * head_masks[0] + state[dv:] * head_masks[1]
        chip_state[...] = packed.astype(jnp.bfloat16)
        chip_total[...] = before[...]
        mate_copy(0).start()
        mate_copy(1).start()

    def scan_copies(step):
        there = {"ep_0": lax.rem(z + (1 if step == 0 else reaches[step - 1]), nz)}
        return [
            pltpu.make_async_remote_copy(
                a.at[step], b.at[step], scan_send.at[step, n], scan_recv.at[step, n],
                device_id=there, device_id_type=MESH,
            )
            for n, (a, b) in enumerate(
                ((scan_out, scan_in), (scan_total_out, scan_total_in))
            )
        ]

    def scan_start(step):
        scan_out[step] = prefix[...].astype(jnp.bfloat16)
        scan_total_out[step] = prefix_total[...]
        for copy in scan_copies(step):
            copy.start()

    def scan_open():
        mate_copy(0).wait_recv()
        mate_copy(1).wait_recv()
        early = core == 0
        own, own_total = chip_state[...].astype(jnp.float32), chip_total[...]
        far, far_total = mate_state[...].astype(jnp.float32), mate_total[...]
        later_total = jnp.where(early, far_total[0:1], own_total[0:1])
        joined = jnp.exp(later_total) * jnp.where(early, own, far) + jnp.where(early, far, own)
        prefix[...] = jnp.where(early, joined[: dv // 2], joined[dv // 2 :])
        prefix_total[...] = own_total + far_total
        scan_start(0)

    def scan_step(step):
        for copy in scan_copies(step):
            copy.wait_recv()
        came = scan_in[step].astype(jnp.float32)
        came_total = scan_total_in[step]
        if step == 0:
            valid = z >= 1
            prefix[...] = jnp.where(valid, came, 0.0)
            prefix_total[...] = jnp.where(valid, came_total, 0.0)
        else:
            valid = z >= reaches[step - 1]
            joined = jnp.exp(prefix_total[0:1]) * came + prefix[...]
            prefix[...] = jnp.where(valid, joined, prefix[...])
            prefix_total[...] = jnp.where(
                valid, prefix_total[...] + came_total, prefix_total[...]
            )
        if step < len(reaches):
            scan_start(step + 1)
        else:
            mine = prefix[...].astype(jnp.bfloat16)
            scan_out[step + 1] = mine
            entering[pl.ds(pl.multiple_of(core * (dv // 2), dv // 2), dv // 2)] = mine
            mate_copy(2).start()

    def finish_mixer():
        mate_half_landed().wait_recv()
        come = entering[...].astype(jnp.float32)
        behind = jnp.exp(mate_total[0:1]) * come + mate_state[...].astype(jnp.float32)
        come = jnp.where(core == 0, come, behind)
        spread_sent(0)
        wide = jnp.concatenate([come * m for m in head_masks], axis=0).astype(jnp.bfloat16)

        @pl.loop(0, nx)
        def _(b):
            span = row_block(b)
            attended = inner[span] + lax.dot_general(
                carried[span], wide, (((1,), (1,)), ((), ())), preferred_element_type=jnp.float32
            )
            heads = []
            for h in range(2):
                one = attended[:, h * dv : (h + 1) * dv]
                inverse = lax.rsqrt(jnp.mean(one * one, axis=-1, keepdims=True) + epsilon)
                heads.append((one * inverse * gain_ref[...]).astype(jnp.bfloat16))
            mix_part[span] = jnp.dot(
                jnp.concatenate(heads, axis=1), mixout_ref[...], preferred_element_type=jnp.float32
            ).astype(jnp.bfloat16)

        fold_start(0)

    def shared():
        @pl.loop(0, nx // 2)
        def _(n):
            span = pl.ds(pl.multiple_of(n * 2 * tokens, 2 * tokens), 2 * tokens)
            rows = exp_all[span]
            gate = jnp.dot(rows, sgate_ref[...], preferred_element_type=jnp.float32)
            lift = jnp.dot(rows, slift_ref[...], preferred_element_type=jnp.float32)
            unit = (gate / (1.0 + jnp.exp(-gate)) * lift).astype(jnp.bfloat16)
            exp_part[span] = jnp.dot(
                unit, sdrop_ref[...], preferred_element_type=jnp.float32
            ).astype(jnp.bfloat16)

    spread_start(0)
    for c in range(2):
        for way in range(2):
            gather_copy(1, way, c).start()
    for way in range(2):
        meta_copy(1, way).start()

    def pass_rows(k, c):
        for way in range(2):
            gather_copy(k, way, c).wait_recv()
            if not (isinstance(k, int) and k == half - 1) or way == c:
                gather_copy(k + 1, way, c).start()

    def pass_meta(k):
        for way in range(2):
            meta_copy(k, way).wait_recv()
            if not (isinstance(k, int) and k == half - 1) or way == 0:
                meta_copy(k + 1, way).start()

    last = half - 1
    blocks = mix_all.shape[0] // BLOCK
    for c in range(2):
        pass_rows(1, c)
    pass_meta(1)
    dispatch(1)
    for load in loads:
        load.wait()
    spread_turn(0)

    @pl.loop(2, last)
    def _(k):
        pass_rows(k, 0)

        @pl.when(k == 2)
        def _():
            spread_end(0)
            project()
            spread_start(1)

        @pl.when((k == 3) | (k == 4))
        def _():
            scan_blocks((k - 3) * (blocks // 2), (k - 2) * (blocks // 2))

        @pl.when(k == 4)
        def _():
            states_out()

        @pl.when(k == 5)
        def _():
            scan_open()
            spread_end(1)
            shared()

        @pl.when(k == 6)
        def _():
            scan_step(0)

        pass_rows(k, 1)
        pass_meta(k)
        dispatch(k)
        experts_on(k - 1)

        @pl.when(k == 3)
        def _():
            spread_turn(1)

    pass_rows(last, 0)
    scan_step(1)
    pass_rows(last, 1)
    pass_meta(last)
    dispatch(last)
    experts_on(last - 1)
    for c in range(2):
        gather_copy(half, c, c).wait_recv()
    meta_copy(half, 0).wait_recv()
    dispatch(0)
    experts_on(last)
    back_start(last)
    scan_step(2)
    experts_on(0)
    back_start(0)
    back_start(last - 1)

    def combined(k, span):
        return lax.dot_general(
            picks[k], back[k, :, span], (((0,), (0,)), ((), ())),
            preferred_element_type=jnp.float32,
        )

    def returned(k):
        for i in range(1, peers):
            back_landed(k, i).wait_recv()

    def sum_copy(k, way, c):
        if isinstance(k, int) and k == half:
            source = first.at[:, columns(c)]
        else:
            source = sums.at[way, k, :, columns(c)]
        return pltpu.make_async_remote_copy(
            source, sums.at[way, k - 1, :, columns(c)],
            rs_send.at[way, k, c], rs_recv.at[way, k, c],
            device_id={"ep_0": beside[way]}, device_id_type=MESH,
        )

    returned(0)
    for c in range(2):
        both = combined(0, columns(c))
        own_sum[:, columns(c)] = both[0:tokens]
        first[:, columns(c)] = both[tokens:].astype(jnp.bfloat16)
        sum_copy(half, c, c).start()

    def pass_on(k, c, landed):
        both = combined(k, columns(c))
        for way in range(2):
            part = both[tokens:] if way == 0 else both[0:tokens]
            if landed(way, c):
                sum_copy(k + 1, way, c).wait_recv()
                part = part + sums[way, k, :, columns(c)].astype(jnp.float32)
            sums[way, k, :, columns(c)] = part.astype(jnp.bfloat16)
            sum_copy(k, way, c).start()

    returned(last)
    for c in range(2):
        pass_on(last, c, lambda way, c: way == c)
    back_start(last - 2)
    scan_step(3)
    fold_start(1)

    @pl.loop(1, last)
    def _(n):
        k = last - n
        returned(k)
        for c in range(2):
            pass_on(k, c, lambda way, c: True)

        @pl.when(k >= 3)
        def _():
            back_start(k - 2)

        @pl.when(n == 1)
        def _():
            scan_step(4)

        @pl.when(n == 2)
        def _():
            fold_turn(1)
            finish_mixer()

        @pl.when(n == 4)
        def _():
            fold_turn(0)

    for c in range(2):
        mixed_ref[:, columns(c)] = fold_end(0, c).astype(jnp.bfloat16)
        own_sum[:, columns(c)] += fold_end(1, c)

    for c in range(2):
        total = own_sum[:, columns(c)]
        for way in range(2):
            sum_copy(1, way, c).wait_recv()
            total = total + sums[way, 0, :, columns(c)].astype(jnp.float32)
        out_ref[:, columns(c)] = total.astype(jnp.bfloat16)

    spread_sent(1)
    for which in range(2):
        fold_sent(which)
    for part in range(3):
        mate_copy(part).wait_send()
    for number in range(len(reaches) + 1):
        for copy in scan_copies(number):
            copy.wait_send()

    for c in range(2):
        for way in range(2):
            gather_copy(1, way, c).wait_send()
            sum_copy(1, way, c).wait_send()
            if way == c:
                gather_copy(half, way, c).wait_send()
                sum_copy(half, way, c).wait_send()
    for way in range(2):
        meta_copy(1, way).wait_send()
    meta_copy(half, 0).wait_send()

    @pl.loop(2, half)
    def _(k):
        for way in range(2):
            for c in range(2):
                gather_copy(k, way, c).wait_send()
                sum_copy(k, way, c).wait_send()
            meta_copy(k, way).wait_send()

    @pl.loop(0, half)
    def _(k):
        for i in range(1, peers):
            out_copy(k, i).wait_send()
            back_copy(k, i).wait_send()


def fused(
    mesh_sizes, mix_rows, rows, mix_gain, ffn_gain, ids, weights, shift, w_decay, decay_bias,
    head_gain,
    w_gate, w_lift, w_drop, w_query, w_key, w_value, w_lowrank, w_output,
    shared_gate, shared_lift, shared_drop,
):
    nz, nc, nx = mesh_sizes
    half, peers = nz // 2, nc * nx
    tokens, width = rows.shape
    ff = w_gate.shape[-1]
    cap = 2 * tokens * ids.shape[1] // (nz * peers)
    slots = 2 * cap
    span = nx * tokens
    keys, values = w_query.shape[1], w_value.shape[1]
    dv = values * DK // keys
    scans = len([d for d in (1, 2, 4, 8, 16, 32) if d < nz]) + 1
    meta = jnp.concatenate([ids.T.astype(jnp.float32), weights.T], axis=0)
    vmem, dma = pltpu.VMEM, pltpu.SemaphoreType.DMA
    bf, f32 = jnp.bfloat16, jnp.float32
    whole = pl.BlockSpec(memory_space=pltpu.VMEM)
    anywhere = pl.BlockSpec(memory_space=pl.ANY)
    return pl.pallas_call(
        functools.partial(moe_kernel, nz, nc, nx),
        out_shape=(jax.ShapeDtypeStruct((tokens, width), bf),) * 2,
        in_specs=[whole] * 9 + [anywhere] * 11,
        out_specs=(whole, whole),
        scratch_shapes=[
            vmem((half, 2 * tokens, width), bf),
            vmem((half, 16, tokens), f32),
            vmem((half, peers * slots, 2 * tokens), bf),
            vmem((half, peers * slots, width), bf),
            vmem((half, peers * slots, width), bf),
            vmem((half, peers * slots, width), bf),
            vmem((half, peers * slots, width), bf),
            vmem((2, half, tokens, width), bf),
            vmem((tokens, width), bf),
            vmem((width, ff), bf),
            vmem((width, ff), bf),
            vmem((ff, width), bf),
            vmem((width, keys), bf),
            vmem((width, keys), bf),
            vmem((width, values), bf),
            vmem(w_lowrank.shape, bf),
            vmem((values, width), bf),
            vmem(shared_gate.shape, bf),
            vmem(shared_lift.shape, bf),
            vmem(shared_drop.shape, bf),
            vmem((peers * slots, ff), bf),
            vmem((tokens, width), f32),
            vmem((span, width), bf),
            vmem((span, width), bf),
            vmem((span, width), bf),
            vmem((2, 2, tokens, width), bf),
            vmem((2, 2, tokens, width), bf),
            vmem((span, keys), bf),
            vmem((span, keys), bf),
            vmem((span, values), bf),
            vmem((span, keys), f32),
            vmem((span, values), f32),
            vmem((span, keys), bf),
            vmem((values, keys), f32),
            vmem((8, keys), f32),
            vmem((dv, keys), bf),
            vmem((8, keys), f32),
            vmem((dv, keys), bf),
            vmem((8, keys), f32),
            vmem((dv // 2, keys), f32),
            vmem((8, keys), f32),
            vmem((scans + 1, dv // 2, keys), bf),
            vmem((scans, 8, keys), f32),
            vmem((scans, dv // 2, keys), bf),
            vmem((scans, 8, keys), f32),
            vmem((dv, keys), bf),
            dma((2, half + 1, 2)), dma((2, half + 1, 2)),
            dma((2, half + 1)), dma((2, half + 1)),
            dma((half, peers)), dma((half, peers)),
            dma((half, peers)), dma((half, peers)),
            dma((2, half + 1, 2)), dma((2, half + 1, 2)),
            dma((11,)),
            dma((2, 3, 2, 2)), dma((2, 3, 2, 2)),
            dma((2, 3, 2, 2)), dma((2, 3, 2, 2)),
            dma((3,)), dma((3,)),
            dma((scans, 2)), dma((scans, 2)),
        ],
        compiler_params=pltpu.CompilerParams(
            collective_id=0, has_side_effects=True, vmem_limit_bytes=63 * 1024 * 1024
        ),
        cost_estimate=pl.CostEstimate(
            flops=200_000_000_000, bytes_accessed=16 * 2**20, transcendentals=0
        ),
    )(
        mix_rows, rows, mix_gain, ffn_gain, meta, shift, w_decay, decay_bias, head_gain,
        w_gate[0], w_lift[0], w_drop[0], w_query, w_key, w_value, w_lowrank, w_output,
        shared_gate, shared_lift, shared_drop,
    )


def body(
    mix_rows,
    expert_rows,
    mix_gain,
    ffn_gain,
    w_query,
    w_key,
    w_value,
    w_lowrank,
    w_decay,
    decay_bias,
    decay_shift,
    head_gain,
    w_output,
    route_ids,
    route_weights,
    w_gate,
    w_lift,
    w_drop,
    shared_gate,
    shared_lift,
    shared_drop,
):
    sizes = (lax.axis_size("ep_0"), lax.axis_size("ep_1"), lax.axis_size("tp"))
    return fused(
        sizes, mix_rows, expert_rows, mix_gain[None], ffn_gain[None], route_ids, route_weights,
        decay_shift, w_decay, decay_bias[None], head_gain[None], w_gate, w_lift, w_drop,
        w_query, w_key, w_value, jnp.transpose(w_lowrank), w_output,
        shared_gate, shared_lift, shared_drop,
    )


def solution(mesh):
    finer = Mesh(
        mesh.devices.reshape(mesh.shape["grp"], 16, 2, mesh.shape["tp"]),
        ("grp", "ep_0", "ep_1", "tp"),
    )
    in_specs = (
        P(GRP_EP_TP, None),
        P(GRP_EP_TP, None),
        P(),
        P(),
        P(None, "tp"),
        P(None, "tp"),
        P(None, "tp"),
        P(),
        P(),
        P(),
        P("tp", GRP_EP),
        P(),
        P("tp", None),
        P(GRP_EP_TP, None),
        P(GRP_EP_TP, None),
        P(EP_TP, None, None),
        P(EP_TP, None, None),
        P(EP_TP, None, None),
        P(None, "tp"),
        P(None, "tp"),
        P("tp", None),
    )
    out_specs = (P(GRP_EP_TP, None), P(GRP_EP_TP, None))
    return jax.shard_map(body, mesh=finer, in_specs=in_specs, out_specs=out_specs, check_vma=False)
```
